256 devices in a mesh: fs: 32 (over z, y), tp: 8 (over x, core).
Axes of the slice: x: 4, y: 4, z: 8, core: 2. Of those that a mesh axis runs over, the one named last changes fastest.
Arguments:
- layer_input: bfloat16 [65536, 2048], P('fs'), may hold values from -6 to 6
- input_cotangent: bfloat16 [65536, 2048], P('fs', 'tp'), may hold values from -6 to 6
- gate_cotangent: bfloat16 [65536, 2048], P('fs', 'tp'), may hold values from -6 to 6
- input_weight: float32 [2048, 2048], P('fs', 'tp'), may hold values from -0.125 to 0.125
- gate_weight: float32 [2048, 2048], P('fs', 'tp'), may hold values from -0.125 to 0.125
- input_basis: bfloat16 [2048, 256], P('fs'), may hold values from -1.81196113 to 1.81196113
- gate_basis: bfloat16 [2048, 256], P('fs'), may hold values from -1.81196113 to 1.81196113
- input_first: float32 [256, 2048], P('fs', 'tp'), may hold values from -20992 to 20992
- input_second: float32 [256, 2048], P('fs', 'tp'), may hold values from 65536 to 1966080
- gate_first: float32 [256, 2048], P('fs', 'tp'), may hold values from -20992 to 20992
- gate_second: float32 [256, 2048], P('fs', 'tp'), may hold values from 65536 to 1966080
Outputs:
- input_new: float32 [2048, 2048], P('fs', 'tp')
- gate_new: float32 [2048, 2048], P('fs', 'tp')
- input_step: float32 [2048, 2048], P('fs', 'tp')
- gate_step: float32 [2048, 2048], P('fs', 'tp')
- input_first_new: float32 [256, 2048], P('fs', 'tp')
- input_second_new: float32 [256, 2048], P('fs', 'tp')
- gate_first_new: float32 [256, 2048], P('fs', 'tp')
- gate_second_new: float32 [256, 2048], P('fs', 'tp')
- input_copy: bfloat16 [2048, 2048], P(None, 'tp')
- gate_copy: bfloat16 [2048, 2048], P(None, 'tp')
The draws below stay inside these ranges and needn't reach their ends.
All inputs are finite; a program needn't handle non-finite values.
Results may differ from the reference program's by a relative error of at most 0.0055.
Values may be sent and summed in bfloat16 or wider, within the bound.
A program may use at most 64 MiB of HBM per device.

```python
import math
import jax
import jax.numpy as jnp
from jax import lax

D = 2048
W = 2048
RANK = 256
TOKENS = 65536


def basis_draw(key):
    base_key, rough_key = jax.random.split(key)
    base = jnp.clip(jax.random.normal(base_key, (D, RANK), jnp.float32), -6.0, 6.0)
    spread = math.log(10.0)
    position = jnp.arange(D, dtype=jnp.float32) / max(D - 1, 1)
    rough = jax.random.uniform(rough_key, (D, 1), jnp.float32, -0.3, 0.3)
    scale = jnp.exp(spread * position[:, None] + rough) / math.sqrt(D)
    return (base * scale).astype(jnp.bfloat16)


def moment_draw(key):
    base_key, rough_key = jax.random.split(key)
    base = jnp.clip(jax.random.normal(base_key, (RANK, W), jnp.float32), -6.0, 6.0)
    spread = math.log(10.0)
    position = jnp.arange(W, dtype=jnp.float32) / max(W - 1, 1)
    rough = jax.random.uniform(rough_key, (1, W), jnp.float32, -0.3, 0.3)
    scale = jnp.exp(spread * position[None, :] + rough) * math.sqrt(TOKENS)
    return base * scale


def draw_input_basis(key, part):
    return basis_draw(jax.random.fold_in(key, 11))


def draw_gate_basis(key, part):
    return basis_draw(jax.random.fold_in(key, 12))


def draw_input_first(key, part):
    return moment_draw(jax.random.fold_in(key, 21))


def draw_gate_first(key, part):
    return moment_draw(jax.random.fold_in(key, 22))


def shard_levels(key, dims, cuts, low, largest):
    factor_of, own = 1.0, jax.random.fold_in(key, 6)
    for dim, blocks in cuts:
        heights = jnp.exp(jax.random.uniform(jax.random.fold_in(own, dim), (blocks,), jnp.float32, low / len(cuts), largest / len(cuts)))
        factor_of = factor_of * jnp.repeat(heights, dims[dim] // blocks).reshape([-1 if axis == dim else 1 for axis in range(len(dims))])
    return factor_of


def scatter_about(rng, extent, scale, reach, cuts=(), kind=jnp.bfloat16):
    result = scale * jax.random.normal(rng, extent, jnp.float32)
    if cuts:
        result = result * shard_levels(rng, extent, cuts, -0.22, 0.18)
    return jnp.clip(result, -reach, reach).astype(kind)


def setup_inputs(seed: int = 0) -> dict:
    splits = jax.random.split(jax.random.key(seed), 12)
    layer_input = scatter_about(splits[0], (TOKENS, D), 1.0, 6.0, ((0, 32),))
    input_cotangent = scatter_about(splits[1], (TOKENS, W), 1.0, 6.0, ((0, 32), (1, 8)))
    gate_cotangent = scatter_about(splits[2], (TOKENS, W), 1.0, 6.0, ((0, 32), (1, 8)))
    input_weight = scatter_about(splits[3], (D, W), D ** -0.5, 0.125, ((0, 32), (1, 8)), jnp.float32)
    gate_weight = scatter_about(splits[4], (D, W), D ** -0.5, 0.125, ((0, 32), (1, 8)), jnp.float32)
    input_basis = draw_input_basis(jax.random.fold_in(splits[11], 71), 0)
    gate_basis = draw_gate_basis(jax.random.fold_in(splits[11], 71), 0)
    input_first = draw_input_first(jax.random.fold_in(splits[11], 71), 0)
    input_second = jnp.clip(jnp.exp(math.log(1966080) - 3.4011974 * jax.random.uniform(splits[8], (RANK, W), jnp.float32) ** shard_levels(splits[8], (RANK, W), ((0, 32), (1, 8)), -0.2, 0.2)), 65536.0, 1966080)
    gate_first = draw_gate_first(jax.random.fold_in(splits[11], 71), 0)
    gate_second = jnp.clip(jnp.exp(math.log(1966080) - 3.4011974 * jax.random.uniform(splits[10], (RANK, W), jnp.float32) ** shard_levels(splits[10], (RANK, W), ((0, 32), (1, 8)), -0.2, 0.2)), 65536.0, 1966080)
    return dict(layer_input=layer_input, input_cotangent=input_cotangent, gate_cotangent=gate_cotangent, input_weight=input_weight, gate_weight=gate_weight, input_basis=input_basis, gate_basis=gate_basis, input_first=input_first, input_second=input_second, gate_first=gate_first, gate_second=gate_second)


first_decay = 0.8
second_decay = 0.95
learn_rate = 0.01

def update_one(layer_input, cotangent, weight, basis, first, second):
    gradient = lax.dot_general(layer_input, cotangent, (((0,), (0,)), ((), ())), preferred_element_type=jnp.float32)
    small = jnp.dot(basis.astype(jnp.float32).T, gradient, precision=lax.Precision.HIGHEST)
    first_new = first_decay * first + (1.0 - first_decay) * small
    second_new = second_decay * second + (1.0 - second_decay) * small * small
    direction = (first_new / (jnp.sqrt(second_new) + 1e-08)).astype(jnp.bfloat16)
    update = jnp.dot(basis, direction, preferred_element_type=jnp.float32)
    spread = jnp.sqrt(jnp.sum(update * update) / (D * W) + 1e-06)
    factor = jnp.minimum(1.0, 1.0 / spread)
    step = factor * update
    fresh = weight - learn_rate * step
    return (fresh, step, first_new, second_new, fresh.astype(jnp.bfloat16))

def reference(layer_input, input_cotangent, gate_cotangent, input_weight, gate_weight, input_basis, gate_basis, input_first, input_second, gate_first, gate_second):
    in_new, in_step, in_first, in_second, in_copy = update_one(layer_input, input_cotangent, input_weight, input_basis, input_first, input_second)
    gt_new, gt_step, gt_first, gt_second, gt_copy = update_one(layer_input, gate_cotangent, gate_weight, gate_basis, gate_first, gate_second)
    return (in_new, gt_new, in_step, gt_step, in_first, in_second, gt_first, gt_second, in_copy, gt_copy)
```

```python
import functools

import jax
import jax.numpy as jnp
from jax import lax
from jax.experimental import pallas as pl
from jax.experimental.pallas import tpu as pltpu
from jax.sharding import Mesh
from jax.sharding import PartitionSpec as P

FS = ("fs_0", "fs_1")
TP = ("tp_0", "tp_1")
MESH = pl.DeviceIdType.MESH
F32, BF16 = jnp.float32, jnp.bfloat16

first_decay = 0.8
second_decay = 0.95
learn_rate = 0.01


ARGS = ("x_in", "ci_in", "cg_in", "wi_in", "wg_in", "bi_in", "bg_in", "fi_in", "si_in", "fg_in", "sg_in")
OUTS = ("ni_out", "ng_out", "ti_out", "tg_out", "fi_out", "si_out", "fg_out", "sg_out", "ki_out", "kg_out")


def scratch(nz, ny, nx, tokens):
    rank, cols, rows = nz * ny * 8, 256, ny * 64
    vmem = {
        "xb": ((nz, tokens, rows), BF16),
        "cb": ((2, tokens, cols), BF16),
        "ct": ((2, cols, tokens), BF16),
        "gh": ((nz, 2, cols, rows), BF16),
        "gl": ((nz, 2, cols, rows), BF16),
        "st": ((2, cols, rank), F32),
        "bb": ((2, nz, ny, nx, 64 // nx, rank), BF16),
        "wf": ((2, 64, cols), F32),
        "wb": ((2, nz, ny, 64, cols), BF16),
        "mo": ((4, 8, cols), F32),
        "mn": ((4, 8, cols), F32),
        "sb": ((nz, ny, 16, cols), BF16),
        "ry": ((ny - 1, nz, 16, cols), BF16),
        "tz": ((nz, 16, cols), BF16),
        "rz": ((nz - 1, 16, cols), BF16),
        "db": ((nz, ny, 16, cols), BF16),
        "dd": ((2, rank, cols), BF16),
        "up": ((2, nz, rows, cols), F32),
        "ss": ((2 * nx, 8, 128), F32),
        "ob": ((2, 2, 64, cols), F32),
        "ck": ((2, nz, rows, cols), BF16),
    }
    sems = {
        "x_sem": (nz,), "c_sem": (2,), "w_sem": (2,), "b_sem": None, "m_sem": (4,), "out_sem": (10,),
        "z_recv": (nz,), "mid_recv": (nz,), "last_recv": (nz,), "core_recv": (nz,),
        "ring_recv": (2, 2, nz // 2 + 1), "wy_recv": None, "ay_recv": None, "az_recv": None,
        "dz_recv": None, "dy_recv": None, "ss_recv": None, "send": (11,),
    }
    names = tuple(vmem) + tuple(sems)
    dma = pltpu.SemaphoreType.DMA
    shapes = [pltpu.VMEM(*v) for v in vmem.values()] + [dma if v is None else dma(v) for v in sems.values()]
    return names, shapes


def update_kernel(nz, ny, nx, entries, names, *refs):
    r = dict(zip(ARGS + OUTS + names, refs))
    x_in, ci_in, cg_in, wi_in, wg_in, bi_in, bg_in, fi_in, si_in, fg_in, sg_in = (r[n] for n in ARGS)
    ni_out, ng_out, ti_out, tg_out, fi_out, si_out, fg_out, sg_out, ki_out, kg_out = (r[n] for n in OUTS)
    (
        xb, cb, ct, gh, gl, st, bb, wf, wb, mo, mn, sb, ry, tz, rz, db, dd, up, ss, ob, ck,
        x_sem, c_sem, w_sem, b_sem, m_sem, out_sem, z_recv, mid_recv, last_recv, core_recv,
        ring_recv, wy_recv, ay_recv, az_recv, dz_recv, dy_recv, ss_recv, send,
    ) = (r[n] for n in names)
    slab, rows, rank = 64 // nx, ny * 64, st.shape[2]
    z, y = lax.axis_index("fs_0"), lax.axis_index("fs_1")
    x, c = lax.axis_index("tp_0"), lax.axis_index("tp_1")
    me_tp = x * 2 + c
    own_l = y * (1 - c) + x * c
    own_m = x * (1 - c) + y * c

    def zz_of(k):
        sign = 2 * lax.rem(k, 2) - 1 if not isinstance(k, int) else 2 * (k % 2) - 1
        return lax.rem(z + sign * ((k + 1) // 2) + nz, nz)

    def peer_z(d):
        return {"fs_0": lax.rem(z + d, nz)}

    def peer_y(d):
        return {"fs_1": lax.rem(y + d, ny)}

    def peer_mid(d):
        return {"fs_1": lax.rem(y + d * c, ny), "tp_0": lax.rem(x + d * (1 - c), nx)}

    def peer_last(d):
        return {"fs_1": lax.rem(y + d * (1 - c), ny), "tp_0": lax.rem(x + d * c, nx)}

    def push(src, dst, s, recv, device):
        pltpu.make_async_remote_copy(
            src_ref=src, dst_ref=dst, send_sem=send.at[s], recv_sem=recv,
            device_id=device, device_id_type=MESH,
        ).start()

    def drain(ref, sem):
        pltpu.make_async_copy(ref, ref, sem).wait()

    def pull(src, dst, sem):
        pltpu.make_async_copy(src, dst, sem).start()

    barrier = pltpu.get_barrier_semaphore()
    peers = [peer_z(d) for d in range(1, nz)] + [peer_y(d) for d in range(1, ny)]
    peers += [{"tp_0": lax.rem(x + d, nx), "tp_1": cc} for d in range(1, nx) for cc in (0, 1)]
    peers += [{"tp_1": 1 - c}]
    for device in peers:
        pl.semaphore_signal(barrier, inc=1, device_id=device, device_id_type=MESH)

    @pl.when(c == 0)
    def _():
        pull(bi_in.at[pl.ds(x * slab, slab)], bb.at[0, z, y, x], b_sem)

    @pl.when(c == 1)
    def _():
        pull(bg_in.at[pl.ds(x * slab, slab)], bb.at[1, z, x, y], b_sem)

    pull(wi_in, wf.at[0], w_sem.at[0])
    pull(wg_in, wf.at[1], w_sem.at[1])
    pull(ci_in, cb.at[0], c_sem.at[0])
    pull(cg_in, cb.at[1], c_sem.at[1])
    for k in range(nz):
        zz = zz_of(k)
        pull(x_in.at[:, pl.ds(pl.multiple_of(zz * rows, 128), rows)], xb.at[k], x_sem.at[k])
    for i, ref in enumerate((fi_in, si_in, fg_in, sg_in)):
        pull(ref, mo.at[i], m_sem.at[i])

    for p in range(2):
        drain(wf.at[p], w_sem.at[p])
        wb[p, z, y] = wf[p].astype(BF16)
    drain(bb.at[c, z, own_l, own_m], b_sem)
    tokens = cb.shape[1]
    chunk = min(256, tokens)
    for p in range(2):
        drain(cb.at[p], c_sem.at[p])

        def flip(i, _):
            at = pl.ds(pl.multiple_of(i * chunk, chunk), chunk)
            ct[p, :, at] = cb[p, at, :].T
            return 0

        lax.fori_loop(0, tokens // chunk, flip, 0)

    pl.semaphore_wait(barrier, len(peers))

    def mid_sends(k):
        zz = zz_of(k)
        for d in range(1, nx):
            block = bb.at[c, zz, own_l, own_m]
            push(block, block, 1, mid_recv.at[k], peer_mid(d))

    def last_sends(k):
        zz = zz_of(k)
        for d in range(1, ny):
            block = bb.at[c, zz, own_l]
            push(block, block, 2, last_recv.at[k], peer_last(d))

    def z_duty(k):
        drain(bb.at[c, zz_of(k), own_l, own_m], z_recv.at[k])
        mid_sends(k)

    def mid_duty(k):
        drain(bb.at[c, zz_of(k), own_l, pl.ds(0, nx - 1)], mid_recv.at[k])
        last_sends(k)

    own = bb.at[c, z, own_l, own_m]
    for k in range(1, nz):
        sign, half = 2 * (k % 2) - 1, (k + 1) // 2
        at_peer = nz - 1 if k == nz - 1 else (k + 1 if k % 2 else k - 1)
        push(own, own, 0, z_recv.at[at_peer], peer_z((sign * half) % nz))
    mid_sends(0)
    for d in range(1, ny):
        push(wb.at[:, z, y], wb.at[:, z, y], 3, wy_recv, peer_y(d))

    def grad_step(k, _):
        drain(xb.at[k], x_sem.at[k])
        for p in range(2):
            g = jnp.dot(ct[p], xb[k], preferred_element_type=F32)
            hi = g.astype(BF16)
            gh[k, p] = hi
            gl[k, p] = (g - hi.astype(F32)).astype(BF16)

        @pl.when(k >= 2)
        def _():
            z_duty(k - 1)

        @pl.when(k >= 3)
        def _():
            mid_duty(k - 3)

        return 0

    lax.fori_loop(0, nz, grad_step, 0)
    for k in range(max(1, nz - 1), nz):
        z_duty(k)
    for k in range(max(0, nz - 3), nz):
        mid_duty(k)

    def ring_reach(p, way):
        return nz // 2 if p == way else nz - 1 - nz // 2

    def ring_block(p, way, s):
        return wb.at[p, lax.rem(z - s + nz if way == 0 else z + s, nz)]

    def ring_send(s):
        for p in range(2):
            for way in range(2):
                if s <= ring_reach(p, way):
                    block = ring_block(p, way, s - 1)
                    push(block, block, 4, ring_recv.at[p, way, s], peer_z(1 if way == 0 else nz - 1))

    def ring_wait(s):
        for p in range(2):
            for way in range(2):
                if s <= ring_reach(p, way):
                    drain(ring_block(p, way, s), ring_recv.at[p, way, s])

    drain(wb.at[:, z, pl.ds(0, ny - 1)], wy_recv)
    ring_send(1)

    def basis(p, j):
        if p == 0:
            return bb[0, j].reshape(rows, rank)
        b = bb[1, j]
        return jnp.concatenate([b[l, m] for m in range(ny) for l in range(nx)], axis=0)

    def core_send(k):
        zz = zz_of(k)
        drain(bb.at[c, zz, pl.ds(0, ny - 1)], last_recv.at[k])
        push(bb.at[c, zz], bb.at[c, zz], 5, core_recv.at[k], {"tp_1": 1 - c})

    def small_step(k):
        zz = zz_of(k)
        drain(bb.at[1 - c, zz], core_recv.at[k])
        for p in range(2):
            b = basis(p, zz)
            st[p] += jnp.dot(gh[k, p], b, preferred_element_type=F32) + jnp.dot(
                gl[k, p], b, preferred_element_type=F32
            )

    st[...] = jnp.zeros_like(st)
    core_send(0)

    def body(k, _):
        core_send(k + 1)
        small_step(k)
        return 0

    lax.fori_loop(0, nz - 1, body, 0)
    small_step(nz - 1)

    parts = [st[p].T.reshape(rank // 8, 8, st.shape[1]) for p in range(2)]
    sb[...] = jnp.concatenate(parts, axis=1).astype(BF16).reshape(sb.shape)
    for d in range(1, ny):
        yy = lax.rem(y + d, ny)
        push(sb.at[:, yy], ry.at[d - 1], 6, ay_recv, peer_y(d))
    if nz > 2:
        ring_wait(1)
        ring_send(2)
    drain(ry, ay_recv)
    total = sb[:, y].astype(F32)
    for d in range(1, ny):
        total += ry[d - 1].astype(F32)
    tz[...] = total.astype(BF16)
    for d in range(1, nz):
        push(tz.at[lax.rem(z + d, nz)], rz.at[d - 1], 7, az_recv, peer_z(d))
    drain(rz, az_recv)
    small = tz[z].astype(F32)
    for d in range(1, nz):
        small += rz[d - 1].astype(F32)

    for i in range(4):
        drain(mo.at[i], m_sem.at[i])
    first = jnp.concatenate([mo[0], mo[2]], axis=0)
    second = jnp.concatenate([mo[1], mo[3]], axis=0)
    first_new = first_decay * first + (1.0 - first_decay) * small
    second_new = second_decay * second + (1.0 - second_decay) * small * small
    db[z, y] = (first_new / (jnp.sqrt(second_new) + 1e-08)).astype(BF16)
    for d in range(1, nz):
        push(db.at[z, y], db.at[z, y], 8, dz_recv, peer_z(d))
    mn[0], mn[1] = first_new[:8], second_new[:8]
    mn[2], mn[3] = first_new[8:], second_new[8:]
    for i, ref in enumerate((fi_out, si_out, fg_out, sg_out)):
        pull(mn.at[i], ref, out_sem.at[i])
    if nz > 2:
        ring_wait(2)
        for s in (3,):
            if s <= nz // 2:
                ring_send(s)
    drain(db.at[pl.ds(0, nz - 1), y], dz_recv)
    for d in range(1, ny):
        push(db.at[:, y], db.at[:, y], 9, dy_recv, peer_y(d))
    if nz > 4:
        ring_wait(3)
        ring_send(4)
    drain(db.at[:, pl.ds(0, ny - 1)], dy_recv)

    directions = db[...].reshape(nz * ny, 16, db.shape[3]).astype(F32)
    halves = [directions[:, 8 * p : 8 * p + 8].reshape(rank, -1).astype(BF16) for p in range(2)]
    for p in range(2):
        dd[p] = halves[p]

    def update_step(j, sums):
        out = []
        for p in range(2):
            u = jnp.dot(basis(p, j), dd[p], preferred_element_type=F32)
            up[p, j] = u
            out.append(sums[p] + jnp.sum((u * u).reshape(-1, 8, u.shape[1]), axis=0))
        return tuple(out)

    zero = jnp.zeros((8, up.shape[3]), F32)
    sums = lax.fori_loop(0, nz, update_step, (zero, zero))
    row = lax.broadcasted_iota(jnp.int32, (8, 128), 0)
    ss[me_tp] = jnp.where(row == 0, jnp.sum(sums[0]), jnp.sum(sums[1]))
    mine = ss.at[me_tp]
    for d in range(1, nx):
        for cc in (0, 1):
            push(mine, mine, 10, ss_recv, {"tp_0": lax.rem(x + d, nx), "tp_1": cc})
    push(mine, mine, 10, ss_recv, {"tp_1": 1 - c})
    ring_wait(nz // 2)
    drain(ss.at[pl.ds(0, 2 * nx - 1)], ss_recv)
    squares = ss[0]
    for t in range(1, 2 * nx):
        squares += ss[t]
    factor = jnp.minimum(1.0, 1.0 / jnp.sqrt(squares / entries + 1e-06))
    factors = (factor[0, 0], factor[1, 0])

    def copy_step(j, _):
        for p in range(2):
            step = factors[p] * up[p, j]
            ck[p, j] = (wb[p, j].reshape(step.shape).astype(F32) - learn_rate * step).astype(BF16)
        for p, ref in enumerate((ki_out, kg_out)):
            pull(ck.at[p, j], ref.at[pl.ds(pl.multiple_of(j * rows, rows), rows)], out_sem.at[8 + p])
        return 0

    lax.fori_loop(0, nz, copy_step, 0)
    for p in range(2):
        step = factors[p] * up[p, z, pl.ds(pl.multiple_of(y * 64, 64), 64), :]
        ob[p, 0] = wf[p] - learn_rate * step
        ob[p, 1] = step
        pull(ob.at[p, 0], (ni_out, ng_out)[p], out_sem.at[4 + 2 * p])
        pull(ob.at[p, 1], (ti_out, tg_out)[p], out_sem.at[5 + 2 * p])
    for p in range(2):
        drain(ob.at[p, 0], out_sem.at[4 + 2 * p])
        drain(ob.at[p, 1], out_sem.at[5 + 2 * p])
        drain(ck.at[p], out_sem.at[8 + p])
    for i in range(4):
        drain(mn.at[i], out_sem.at[i])

    drain(bb.at[c, pl.ds(0, nz - 1), 0, 0], send.at[0])
    drain(bb.at[c, :, pl.ds(0, nx - 1), 0], send.at[1])
    drain(bb.at[c, :, pl.ds(0, ny - 1)], send.at[2])
    drain(wb.at[:, z, pl.ds(0, ny - 1)], send.at[3])
    drain(wb.at[:, pl.ds(0, nz - 1)], send.at[4])
    drain(bb.at[c], send.at[5])
    drain(ry, send.at[6])
    drain(rz, send.at[7])
    drain(db.at[pl.ds(0, nz - 1), 0], send.at[8])
    drain(db.at[:, pl.ds(0, ny - 1)], send.at[9])
    drain(ss.at[pl.ds(0, 2 * nx - 1)], send.at[10])


def shards(nz, ny, nx, entries, *args):
    names, shapes = scratch(nz, ny, nx, args[0].shape[0])
    w, m = args[3], args[7]
    copy = jax.ShapeDtypeStruct((w.shape[0] * nz * ny, w.shape[1]), BF16)
    outs = [jax.ShapeDtypeStruct(a.shape, F32) for a in (w,) * 4 + (m,) * 4] + [copy, copy]
    anywhere = pl.BlockSpec(memory_space=pl.ANY)
    return tuple(
        pl.pallas_call(
            functools.partial(update_kernel, nz, ny, nx, entries, names),
            out_shape=outs,
            in_specs=[anywhere] * len(args),
            out_specs=[anywhere] * len(outs),
            scratch_shapes=shapes,
            compiler_params=pltpu.CompilerParams(
                collective_id=0, has_side_effects=True, vmem_limit_bytes=56 * 1024 * 1024
            ),
        )(*args)
    )


def build(devices, nz, ny, nx):
    torus = Mesh(devices.reshape(nz, ny, nx, 2), FS + TP)
    entries = float(nz * ny * 64 * nx * 2 * 256)
    sharded, copied = P(FS, TP), P(None, TP)
    in_specs = (P(FS, None), sharded, sharded, sharded, sharded, P(FS, None), P(FS, None)) + (sharded,) * 4
    return jax.shard_map(
        functools.partial(shards, nz, ny, nx, entries),
        mesh=torus,
        in_specs=in_specs,
        out_specs=(sharded,) * 8 + (copied,) * 2,
        check_vma=False,
    )


def solution(mesh):
    return build(mesh.devices, 8, 4, 4)
```

```python
import functools

import jax
import jax.numpy as jnp
from jax import lax
from jax.experimental import pallas as pl
from jax.experimental.pallas import tpu as pltpu
from jax.sharding import Mesh
from jax.sharding import PartitionSpec as P

FS = ("fs_0", "fs_1")
TP = ("tp_0", "tp_1")
MESH = pl.DeviceIdType.MESH
F32, BF16 = jnp.float32, jnp.bfloat16

first_decay = 0.8
second_decay = 0.95
learn_rate = 0.01


ARGS = ("x_in", "ci_in", "cg_in", "wi_in", "wg_in", "bi_in", "bg_in", "fi_in", "si_in", "fg_in", "sg_in")
HELD = ("up", "wb", "wf", "mn", "factor")
OUTS = ("ni_out", "ng_out", "ti_out", "tg_out", "fi_out", "si_out", "fg_out", "sg_out", "ki_out", "kg_out")


def scratch(nz, ny, nx, tokens):
    rank, cols, rows = nz * ny * 8, 256, ny * 64
    vmem = {
        "xb": ((nz, tokens, rows), BF16),
        "cb": ((2, tokens, cols), BF16),
        "ct": ((2, cols, tokens), BF16),
        "gh": ((nz, 2, cols, rows), BF16),
        "gl": ((nz, 2, cols, rows), BF16),
        "st": ((2, cols, rank), F32),
        "bb": ((2, nz, ny, nx, 64 // nx, rank), BF16),
        "mo": ((4, 8, cols), F32),
        "sb": ((nz, ny, 16, cols), BF16),
        "ry": ((ny - 1, nz, 16, cols), BF16),
        "tz": ((nz, 16, cols), BF16),
        "rz": ((nz - 1, 16, cols), BF16),
        "db": ((nz, ny, 16, cols), BF16),
        "dd": ((2, rank, cols), BF16),
        "ss": ((2 * nx, 8, 128), F32),
    }
    sems = {
        "x_sem": (nz,), "c_sem": (2,), "w_sem": (2,), "b_sem": None, "m_sem": (4,),
        "z_recv": (nz,), "mid_recv": (nz,), "last_recv": (nz,), "core_recv": (nz,),
        "ring_recv": (2, 2, nz // 2 + 1), "wy_recv": None, "ay_recv": None, "az_recv": None,
        "dz_recv": None, "dy_recv": None, "ss_recv": None, "send": (11,),
    }
    held = {
        "up": ((2, nz, rows, cols), F32),
        "wb": ((2, nz, ny, 64, cols), BF16),
        "wf": ((2, 64, cols), F32),
        "mn": ((4, 8, cols), F32),
        "factor": ((8, 128), F32),
    }
    names = tuple(vmem) + tuple(sems)
    dma = pltpu.SemaphoreType.DMA
    shapes = [pltpu.VMEM(*v) for v in vmem.values()] + [dma if v is None else dma(v) for v in sems.values()]
    return names, shapes, [pltpu.VMEM(*v) for v in held.values()]


def update_kernel(nz, ny, nx, entries, names, *refs):
    r = dict(zip(ARGS + HELD + names, refs))
    x_in, ci_in, cg_in, wi_in, wg_in, bi_in, bg_in, fi_in, si_in, fg_in, sg_in = (r[n] for n in ARGS)
    up, wb, wf, mn, factor = (r[n] for n in HELD)
    (
        xb, cb, ct, gh, gl, st, bb, mo, sb, ry, tz, rz, db, dd, ss,
        x_sem, c_sem, w_sem, b_sem, m_sem, z_recv, mid_recv, last_recv, core_recv,
        ring_recv, wy_recv, ay_recv, az_recv, dz_recv, dy_recv, ss_recv, send,
    ) = (r[n] for n in names)
    slab, rows, rank = 64 // nx, ny * 64, st.shape[2]
    z, y = lax.axis_index("fs_0"), lax.axis_index("fs_1")
    x, c = lax.axis_index("tp_0"), lax.axis_index("tp_1")
    me_tp = x * 2 + c
    own_l = y * (1 - c) + x * c
    own_m = x * (1 - c) + y * c

    def zz_of(k):
        sign = 2 * lax.rem(k, 2) - 1 if not isinstance(k, int) else 2 * (k % 2) - 1
        return lax.rem(z + sign * ((k + 1) // 2) + nz, nz)

    def peer_z(d):
        return {"fs_0": lax.rem(z + d, nz)}

    def peer_y(d):
        return {"fs_1": lax.rem(y + d, ny)}

    def peer_mid(d):
        return {"fs_1": lax.rem(y + d * c, ny), "tp_0": lax.rem(x + d * (1 - c), nx)}

    def peer_last(d):
        return {"fs_1": lax.rem(y + d * (1 - c), ny), "tp_0": lax.rem(x + d * c, nx)}

    def push(src, dst, s, recv, device):
        pltpu.make_async_remote_copy(
            src_ref=src, dst_ref=dst, send_sem=send.at[s], recv_sem=recv,
            device_id=device, device_id_type=MESH,
        ).start()

    def drain(ref, sem):
        pltpu.make_async_copy(ref, ref, sem).wait()

    def pull(src, dst, sem):
        pltpu.make_async_copy(src, dst, sem).start()

    barrier = pltpu.get_barrier_semaphore()
    peers = [peer_z(d) for d in range(1, nz)] + [peer_y(d) for d in range(1, ny)]
    peers += [{"tp_0": lax.rem(x + d, nx), "tp_1": cc} for d in range(1, nx) for cc in (0, 1)]
    peers += [{"tp_1": 1 - c}]
    for device in peers:
        pl.semaphore_signal(barrier, inc=1, device_id=device, device_id_type=MESH)

    @pl.when(c == 0)
    def _():
        pull(bi_in.at[pl.ds(x * slab, slab)], bb.at[0, z, y, x], b_sem)

    @pl.when(c == 1)
    def _():
        pull(bg_in.at[pl.ds(x * slab, slab)], bb.at[1, z, x, y], b_sem)

    pull(wi_in, wf.at[0], w_sem.at[0])
    pull(wg_in, wf.at[1], w_sem.at[1])
    pull(ci_in, cb.at[0], c_sem.at[0])
    pull(cg_in, cb.at[1], c_sem.at[1])
    for k in range(nz):
        zz = zz_of(k)
        pull(x_in.at[:, pl.ds(pl.multiple_of(zz * rows, 128), rows)], xb.at[k], x_sem.at[k])
    for i, ref in enumerate((fi_in, si_in, fg_in, sg_in)):
        pull(ref, mo.at[i], m_sem.at[i])

    for p in range(2):
        drain(wf.at[p], w_sem.at[p])
        wb[p, z, y] = wf[p].astype(BF16)
    drain(bb.at[c, z, own_l, own_m], b_sem)
    tokens = cb.shape[1]
    chunk = min(256, tokens)
    for p in range(2):
        drain(cb.at[p], c_sem.at[p])

        def flip(i, _):
            at = pl.ds(pl.multiple_of(i * chunk, chunk), chunk)
            ct[p, :, at] = cb[p, at, :].T
            return 0

        lax.fori_loop(0, tokens // chunk, flip, 0)

    pl.semaphore_wait(barrier, len(peers))

    def mid_sends(k):
        zz = zz_of(k)
        for d in range(1, nx):
            block = bb.at[c, zz, own_l, own_m]
            push(block, block, 1, mid_recv.at[k], peer_mid(d))

    def last_sends(k):
        zz = zz_of(k)
        for d in range(1, ny):
            block = bb.at[c, zz, own_l]
            push(block, block, 2, last_recv.at[k], peer_last(d))

    def z_duty(k):
        drain(bb.at[c, zz_of(k), own_l, own_m], z_recv.at[k])
        mid_sends(k)

    def mid_duty(k):
        drain(bb.at[c, zz_of(k), own_l, pl.ds(0, nx - 1)], mid_recv.at[k])
        last_sends(k)

    own = bb.at[c, z, own_l, own_m]
    for k in range(1, nz):
        sign, half = 2 * (k % 2) - 1, (k + 1) // 2
        at_peer = nz - 1 if k == nz - 1 else (k + 1 if k % 2 else k - 1)
        push(own, own, 0, z_recv.at[at_peer], peer_z((sign * half) % nz))
    mid_sends(0)
    for d in range(1, ny):
        push(wb.at[:, z, y], wb.at[:, z, y], 3, wy_recv, peer_y(d))

    def grad_step(k, _):
        drain(xb.at[k], x_sem.at[k])
        for p in range(2):
            g = jnp.dot(ct[p], xb[k], preferred_element_type=F32)
            hi = g.astype(BF16)
            gh[k, p] = hi
            gl[k, p] = (g - hi.astype(F32)).astype(BF16)

        @pl.when(k >= 2)
        def _():
            z_duty(k - 1)

        @pl.when(k >= 3)
        def _():
            mid_duty(k - 3)

        return 0

    lax.fori_loop(0, nz, grad_step, 0)
    for k in range(max(1, nz - 1), nz):
        z_duty(k)
    for k in range(max(0, nz - 3), nz):
        mid_duty(k)

    def ring_reach(p, way):
        return nz // 2 if p == way else nz - 1 - nz // 2

    def ring_block(p, way, s):
        return wb.at[p, lax.rem(z - s + nz if way == 0 else z + s, nz)]

    def ring_send(s):
        for p in range(2):
            for way in range(2):
                if s <= ring_reach(p, way):
                    block = ring_block(p, way, s - 1)
                    push(block, block, 4, ring_recv.at[p, way, s], peer_z(1 if way == 0 else nz - 1))

    def ring_wait(s):
        for p in range(2):
            for way in range(2):
                if s <= ring_reach(p, way):
                    drain(ring_block(p, way, s), ring_recv.at[p, way, s])

    drain(wb.at[:, z, pl.ds(0, ny - 1)], wy_recv)
    ring_send(1)

    def basis(p, j):
        if p == 0:
            return bb[0, j].reshape(rows, rank)
        b = bb[1, j]
        return jnp.concatenate([b[l, m] for m in range(ny) for l in range(nx)], axis=0)

    def core_send(k):
        zz = zz_of(k)
        drain(bb.at[c, zz, pl.ds(0, ny - 1)], last_recv.at[k])
        push(bb.at[c, zz], bb.at[c, zz], 5, core_recv.at[k], {"tp_1": 1 - c})

    def small_step(k):
        zz = zz_of(k)
        drain(bb.at[1 - c, zz], core_recv.at[k])
        for p in range(2):
            b = basis(p, zz)
            st[p] += jnp.dot(gh[k, p], b, preferred_element_type=F32) + jnp.dot(
                gl[k, p], b, preferred_element_type=F32
            )

    st[...] = jnp.zeros_like(st)
    core_send(0)

    def body(k, _):
        core_send(k + 1)
        small_step(k)
        return 0

    lax.fori_loop(0, nz - 1, body, 0)
    small_step(nz - 1)

    parts = [st[p].T.reshape(rank // 8, 8, st.shape[1]) for p in range(2)]
    sb[...] = jnp.concatenate(parts, axis=1).astype(BF16).reshape(sb.shape)
    for d in range(1, ny):
        yy = lax.rem(y + d, ny)
        push(sb.at[:, yy], ry.at[d - 1], 6, ay_recv, peer_y(d))
    if nz > 2:
        ring_wait(1)
        ring_send(2)
    drain(ry, ay_recv)
    total = sb[:, y].astype(F32)
    for d in range(1, ny):
        total += ry[d - 1].astype(F32)
    tz[...] = total.astype(BF16)
    for d in range(1, nz):
        push(tz.at[lax.rem(z + d, nz)], rz.at[d - 1], 7, az_recv, peer_z(d))
    drain(rz, az_recv)
    small = tz[z].astype(F32)
    for d in range(1, nz):
        small += rz[d - 1].astype(F32)

    for i in range(4):
        drain(mo.at[i], m_sem.at[i])
    first = jnp.concatenate([mo[0], mo[2]], axis=0)
    second = jnp.concatenate([mo[1], mo[3]], axis=0)
    first_new = first_decay * first + (1.0 - first_decay) * small
    second_new = second_decay * second + (1.0 - second_decay) * small * small
    db[z, y] = (first_new / (jnp.sqrt(second_new) + 1e-08)).astype(BF16)
    for d in range(1, nz):
        push(db.at[z, y], db.at[z, y], 8, dz_recv, peer_z(d))
    mn[0], mn[1] = first_new[:8], second_new[:8]
    mn[2], mn[3] = first_new[8:], second_new[8:]
    if nz > 2:
        ring_wait(2)
        for s in (3,):
            if s <= nz // 2:
                ring_send(s)
    drain(db.at[pl.ds(0, nz - 1), y], dz_recv)
    for d in range(1, ny):
        push(db.at[:, y], db.at[:, y], 9, dy_recv, peer_y(d))
    if nz > 4:
        ring_wait(3)
        ring_send(4)
    drain(db.at[:, pl.ds(0, ny - 1)], dy_recv)

    directions = db[...].reshape(nz * ny, 16, db.shape[3]).astype(F32)
    halves = [directions[:, 8 * p : 8 * p + 8].reshape(rank, -1).astype(BF16) for p in range(2)]
    for p in range(2):
        dd[p] = halves[p]

    def update_step(j, sums):
        out = []
        for p in range(2):
            u = jnp.dot(basis(p, j), dd[p], preferred_element_type=F32)
            up[p, j] = u
            out.append(sums[p] + jnp.sum((u * u).reshape(-1, 8, u.shape[1]), axis=0))
        return tuple(out)

    zero = jnp.zeros((8, up.shape[3]), F32)
    sums = lax.fori_loop(0, nz, update_step, (zero, zero))
    row = lax.broadcasted_iota(jnp.int32, (8, 128), 0)
    ss[me_tp] = jnp.where(row == 0, jnp.sum(sums[0]), jnp.sum(sums[1]))
    mine = ss.at[me_tp]
    for d in range(1, nx):
        for cc in (0, 1):
            push(mine, mine, 10, ss_recv, {"tp_0": lax.rem(x + d, nx), "tp_1": cc})
    push(mine, mine, 10, ss_recv, {"tp_1": 1 - c})
    ring_wait(nz // 2)
    drain(ss.at[pl.ds(0, 2 * nx - 1)], ss_recv)
    squares = ss[0]
    for t in range(1, 2 * nx):
        squares += ss[t]
    factor[...] = jnp.minimum(1.0, 1.0 / jnp.sqrt(squares / entries + 1e-06))

    drain(bb.at[c, pl.ds(0, nz - 1), 0, 0], send.at[0])
    drain(bb.at[c, :, pl.ds(0, nx - 1), 0], send.at[1])
    drain(bb.at[c, :, pl.ds(0, ny - 1)], send.at[2])
    drain(wb.at[:, z, pl.ds(0, ny - 1)], send.at[3])
    drain(wb.at[:, pl.ds(0, nz - 1)], send.at[4])
    drain(bb.at[c], send.at[5])
    drain(ry, send.at[6])
    drain(rz, send.at[7])
    drain(db.at[pl.ds(0, nz - 1), 0], send.at[8])
    drain(db.at[:, pl.ds(0, ny - 1)], send.at[9])
    drain(ss.at[pl.ds(0, 2 * nx - 1)], send.at[10])


def finish_kernel(nz, ny, up, wb, wf, mn, factor, *refs):
    outs, (ob, ck, sem) = refs[:10], refs[10:]
    z, y = lax.axis_index("fs_0"), lax.axis_index("fs_1")
    rows = up.shape[2]
    factors = (factor[0, 0], factor[1, 0])

    def put(src, dst, k):
        pltpu.make_async_copy(src, dst, sem.at[k]).start()

    for i in range(4):
        put(mn.at[i], outs[4 + i], 4 + i)
    for p in range(2):
        step = factors[p] * up[p, z, pl.ds(pl.multiple_of(y * 64, 64), 64), :]
        ob[p] = wf[p] - learn_rate * step
        ob[2 + p] = step
    for i in range(4):
        put(ob.at[i], outs[i], i)

    def copy_step(j, _):
        for p in range(2):
            step = factors[p] * up[p, j]
            ck[p, j] = (wb[p, j].reshape(step.shape).astype(F32) - learn_rate * step).astype(BF16)
            put(ck.at[p, j], outs[8 + p].at[pl.ds(pl.multiple_of(j * rows, rows), rows)], 8 + p)
        return 0

    lax.fori_loop(0, nz, copy_step, 0)
    for i in range(4):
        pltpu.make_async_copy(mn.at[i], outs[4 + i], sem.at[4 + i]).wait()
        pltpu.make_async_copy(ob.at[i], outs[i], sem.at[i]).wait()
    for p in range(2):
        pltpu.make_async_copy(ck.at[p], ck.at[p], sem.at[8 + p]).wait()


def shards(nz, ny, nx, entries, *args):
    names, shapes, held = scratch(nz, ny, nx, args[0].shape[0])
    hbm, vmem = pl.BlockSpec(memory_space=pltpu.HBM), pl.BlockSpec(memory_space=pltpu.VMEM)
    kept = pl.pallas_call(
        functools.partial(update_kernel, nz, ny, nx, entries, names),
        out_shape=held,
        in_specs=[hbm] * len(args),
        out_specs=[vmem] * len(held),
        scratch_shapes=shapes,
        compiler_params=pltpu.CompilerParams(
            collective_id=0, has_side_effects=True, vmem_limit_bytes=58 * 1024 * 1024 - 448 * 1024
        ),
    )(*args)
    w, m = args[3], args[7]
    copy = jax.ShapeDtypeStruct((w.shape[0] * nz * ny, w.shape[1]), BF16)
    outs = [jax.ShapeDtypeStruct(a.shape, F32) for a in (w,) * 4 + (m,) * 4] + [copy, copy]
    return tuple(
        pl.pallas_call(
            functools.partial(finish_kernel, nz, ny),
            out_shape=outs,
            in_specs=[vmem] * len(kept),
            out_specs=[hbm] * len(outs),
            scratch_shapes=[
                pltpu.VMEM((4,) + w.shape, F32),
                pltpu.VMEM((2, nz, ny * 64, w.shape[1]), BF16),
                pltpu.SemaphoreType.DMA((10,)),
            ],
            compiler_params=pltpu.CompilerParams(vmem_limit_bytes=16 * 1024 * 1024),
        )(*kept)
    )


def build(devices, nz, ny, nx):
    torus = Mesh(devices.reshape(nz, ny, nx, 2), FS + TP)
    entries = float(nz * ny * 64 * nx * 2 * 256)
    sharded, copied = P(FS, TP), P(None, TP)
    in_specs = (P(FS, None), sharded, sharded, sharded, sharded, P(FS, None), P(FS, None)) + (sharded,) * 4
    return jax.shard_map(
        functools.partial(shards, nz, ny, nx, entries),
        mesh=torus,
        in_specs=in_specs,
        out_specs=(sharded,) * 8 + (copied,) * 2,
        check_vma=False,
    )


def solution(mesh):
    return build(mesh.devices, 8, 4, 4)
```

```python
import functools

import jax
import jax.numpy as jnp
from jax import lax
from jax.experimental import pallas as pl
from jax.experimental.pallas import tpu as pltpu
from jax.sharding import Mesh
from jax.sharding import PartitionSpec as P

FS = ("fs_0", "fs_1")
TP = ("tp_0", "tp_1")
MESH = pl.DeviceIdType.MESH
F32, BF16 = jnp.float32, jnp.bfloat16

first_decay = 0.8
second_decay = 0.95
learn_rate = 0.01


ARGS = ("x_in", "ci_in", "cg_in", "wi_in", "wg_in", "bi_in", "bg_in", "fi_in", "si_in", "fg_in", "sg_in")
HELD = ("up", "wb", "wf", "mn", "factor")
OUTS = ("ni_out", "ng_out", "ti_out", "tg_out", "fi_out", "si_out", "fg_out", "sg_out", "ki_out", "kg_out")


def scratch(nz, ny, nx, tokens):
    rank, cols, rows = nz * ny * 8, 256, ny * 64
    vmem = {
        "xb": ((nz, tokens, rows), BF16),
        "cb": ((2, tokens, cols), BF16),
        "ct": ((2, cols, tokens), BF16),
        "gh": ((nz, 2, cols, rows), BF16),
        "gl": ((nz, 2, cols, rows), BF16),
        "st": ((2, cols, rank), F32),
        "bb": ((2, nz, ny, nx, 64 // nx, rank), BF16),
        "mo": ((4, 8, cols), F32),
        "sb": ((nz, ny, 16, cols), BF16),
        "ry": ((ny - 1, nz, 16, cols), BF16),
        "tz": ((nz, 16, cols), BF16),
        "rz": ((nz - 1, 16, cols), BF16),
        "db": ((nz, ny, 16, cols), BF16),
        "dd": ((2, rank, cols), BF16),
        "gm": ((2, rank, rank), F32),
        "gb": ((2, 2, rank, rank), BF16),
        "ss": ((2 * nx, 8, 128), F32),
    }
    sems = {
        "x_sem": (nz,), "c_sem": (2,), "w_sem": (2,), "b_sem": None, "m_sem": (4,),
        "z_recv": (nz,), "mid_recv": (nz,), "last_recv": (nz,), "core_recv": (nz,),
        "ring_recv": (2, 2, nz // 2 + 1), "wy_recv": None, "ay_recv": None, "az_recv": None,
        "dz_recv": None, "dy_recv": None, "ss_recv": None, "send": (11,),
    }
    held = {
        "up": ((2, nz, rows, cols), F32),
        "wb": ((2, nz, ny, 64, cols), BF16),
        "wf": ((2, 64, cols), F32),
        "mn": ((4, 8, cols), F32),
        "factor": ((8, 128), F32),
    }
    names = tuple(vmem) + tuple(sems)
    dma = pltpu.SemaphoreType.DMA
    shapes = [pltpu.VMEM(*v) for v in vmem.values()] + [dma if v is None else dma(v) for v in sems.values()]
    return names, shapes, [pltpu.VMEM(*v) for v in held.values()]


def update_kernel(nz, ny, nx, entries, names, *refs):
    r = dict(zip(ARGS + HELD + names, refs))
    x_in, ci_in, cg_in, wi_in, wg_in, bi_in, bg_in, fi_in, si_in, fg_in, sg_in = (r[n] for n in ARGS)
    up, wb, wf, mn, factor = (r[n] for n in HELD)
    (
        xb, cb, ct, gh, gl, st, bb, mo, sb, ry, tz, rz, db, dd, gm, gb, ss,
        x_sem, c_sem, w_sem, b_sem, m_sem, z_recv, mid_recv, last_recv, core_recv,
        ring_recv, wy_recv, ay_recv, az_recv, dz_recv, dy_recv, ss_recv, send,
    ) = (r[n] for n in names)
    slab, rows, rank = 64 // nx, ny * 64, st.shape[2]
    z, y = lax.axis_index("fs_0"), lax.axis_index("fs_1")
    x, c = lax.axis_index("tp_0"), lax.axis_index("tp_1")
    me_tp = x * 2 + c
    own_l = y * (1 - c) + x * c
    own_m = x * (1 - c) + y * c

    def far_first(n):
        return sorted(range(1, n), key=lambda d: -min(d, n - d))

    def zz_of(k):
        sign = 2 * lax.rem(k, 2) - 1 if not isinstance(k, int) else 2 * (k % 2) - 1
        return lax.rem(z + sign * ((k + 1) // 2) + nz, nz)

    def peer_z(d):
        return {"fs_0": lax.rem(z + d, nz)}

    def peer_y(d):
        return {"fs_1": lax.rem(y + d, ny)}

    def peer_mid(d):
        return {"fs_1": lax.rem(y + d * c, ny), "tp_0": lax.rem(x + d * (1 - c), nx)}

    def peer_last(d):
        return {"fs_1": lax.rem(y + d * (1 - c), ny), "tp_0": lax.rem(x + d * c, nx)}

    def push(src, dst, s, recv, device):
        pltpu.make_async_remote_copy(
            src_ref=src, dst_ref=dst, send_sem=send.at[s], recv_sem=recv,
            device_id=device, device_id_type=MESH,
        ).start()

    def drain(ref, sem):
        pltpu.make_async_copy(ref, ref, sem).wait()

    def pull(src, dst, sem):
        pltpu.make_async_copy(src, dst, sem).start()

    barrier = pltpu.get_barrier_semaphore()
    peers = [peer_z(d) for d in range(1, nz)] + [peer_y(d) for d in range(1, ny)]
    peers += [{"tp_0": lax.rem(x + d, nx), "tp_1": cc} for d in range(1, nx) for cc in (0, 1)]
    peers += [{"tp_1": 1 - c}]
    for device in peers:
        pl.semaphore_signal(barrier, inc=1, device_id=device, device_id_type=MESH)

    @pl.when(c == 0)
    def _():
        pull(bi_in.at[pl.ds(x * slab, slab)], bb.at[0, z, y, x], b_sem)

    @pl.when(c == 1)
    def _():
        pull(bg_in.at[pl.ds(x * slab, slab)], bb.at[1, z, x, y], b_sem)

    pull(wi_in, wf.at[0], w_sem.at[0])
    pull(wg_in, wf.at[1], w_sem.at[1])
    pull(ci_in, cb.at[0], c_sem.at[0])
    pull(cg_in, cb.at[1], c_sem.at[1])
    for k in range(nz):
        zz = zz_of(k)
        pull(x_in.at[:, pl.ds(pl.multiple_of(zz * rows, 128), rows)], xb.at[k], x_sem.at[k])
    for i, ref in enumerate((fi_in, si_in, fg_in, sg_in)):
        pull(ref, mo.at[i], m_sem.at[i])

    for p in range(2):
        drain(wf.at[p], w_sem.at[p])
        wb[p, z, y] = wf[p].astype(BF16)
    drain(bb.at[c, z, own_l, own_m], b_sem)
    tokens = cb.shape[1]
    chunk = min(256, tokens)
    for p in range(2):
        drain(cb.at[p], c_sem.at[p])

        def flip(i, _):
            at = pl.ds(pl.multiple_of(i * chunk, chunk), chunk)
            ct[p, :, at] = cb[p, at, :].T
            return 0

        lax.fori_loop(0, tokens // chunk, flip, 0)

    pl.semaphore_wait(barrier, len(peers))

    def mid_sends(k):
        zz = zz_of(k)
        for d in far_first(nx):
            block = bb.at[c, zz, own_l, own_m]
            push(block, block, 1, mid_recv.at[k], peer_mid(d))

    def last_sends(k):
        zz = zz_of(k)
        for d in far_first(ny):
            block = bb.at[c, zz, own_l]
            push(block, block, 2, last_recv.at[k], peer_last(d))

    def z_duty(k):
        drain(bb.at[c, zz_of(k), own_l, own_m], z_recv.at[k])
        mid_sends(k)

    def mid_duty(k):
        drain(bb.at[c, zz_of(k), own_l, pl.ds(0, nx - 1)], mid_recv.at[k])
        last_sends(k)

    own = bb.at[c, z, own_l, own_m]
    for k in range(nz - 1, 0, -1):
        sign, half = 2 * (k % 2) - 1, (k + 1) // 2
        at_peer = nz - 1 if k == nz - 1 else (k + 1 if k % 2 else k - 1)
        push(own, own, 0, z_recv.at[at_peer], peer_z((sign * half) % nz))
    mid_sends(0)
    for d in far_first(ny):
        push(wb.at[:, z, y], wb.at[:, z, y], 3, wy_recv, peer_y(d))

    def grad_step(k, _):
        drain(xb.at[k], x_sem.at[k])
        for p in range(2):
            g = jnp.dot(ct[p], xb[k], preferred_element_type=F32)
            hi = g.astype(BF16)
            gh[k, p] = hi
            gl[k, p] = (g - hi.astype(F32)).astype(BF16)
        return 0

    def each(first, last, duty):
        def one(k, _):
            duty(k)
            return 0

        lax.fori_loop(first, last, one, 0)

    cut1, cut2 = (nz * 5) // 8, (nz * 6) // 8
    lax.fori_loop(0, cut1, grad_step, 0)
    each(1, cut1, z_duty)
    mid_duty(0)
    lax.fori_loop(cut1, cut2, grad_step, 0)
    each(cut1, nz, z_duty)
    lax.fori_loop(cut2, nz, grad_step, 0)
    each(1, nz, mid_duty)

    def ring_reach(p, way):
        return nz // 2 if p == way else nz - 1 - nz // 2

    def ring_block(p, way, s):
        return wb.at[p, lax.rem(z - s + nz if way == 0 else z + s, nz)]

    def ring_send(s):
        for p in range(2):
            for way in range(2):
                if s <= ring_reach(p, way):
                    block = ring_block(p, way, s - 1)
                    push(block, block, 4, ring_recv.at[p, way, s], peer_z(1 if way == 0 else nz - 1))

    def ring_wait(s):
        for p in range(2):
            for way in range(2):
                if s <= ring_reach(p, way):
                    drain(ring_block(p, way, s), ring_recv.at[p, way, s])

    drain(wb.at[:, z, pl.ds(0, ny - 1)], wy_recv)
    ring_send(1)

    def basis(p, j):
        if p == 0:
            return bb[0, j].reshape(rows, rank)
        b = bb[1, j]
        return jnp.concatenate([b[l, m] for m in range(ny) for l in range(nx)], axis=0)

    def core_send(k):
        zz = zz_of(k)
        drain(bb.at[c, zz, pl.ds(0, ny - 1)], last_recv.at[k])
        push(bb.at[c, zz], bb.at[c, zz], 5, core_recv.at[k], {"tp_1": 1 - c})

    def small_step(k):
        zz = zz_of(k)
        drain(bb.at[1 - c, zz], core_recv.at[k])
        for p in range(2):
            b = basis(p, zz)
            st[p] += jnp.dot(gh[k, p], b, preferred_element_type=F32) + jnp.dot(
                gl[k, p], b, preferred_element_type=F32
            )

    st[...] = jnp.zeros_like(st)
    core_send(0)

    def body(k, _):
        core_send(k + 1)
        small_step(k)
        return 0

    lax.fori_loop(0, nz - 1, body, 0)
    small_step(nz - 1)

    parts = [st[p].T.reshape(rank // 8, 8, st.shape[1]) for p in range(2)]
    sb[...] = jnp.concatenate(parts, axis=1).astype(BF16).reshape(sb.shape)
    for d in far_first(ny):
        yy = lax.rem(y + d, ny)
        push(sb.at[:, yy], ry.at[d - 1], 6, ay_recv, peer_y(d))
    if nz > 2:
        ring_wait(1)
        ring_send(2)

    gm[...] = jnp.zeros_like(gm)

    def gram_step(j, _):
        for p in range(2):
            b = bb[p, j].reshape(rows, rank)
            gm[p] += lax.dot_general(b, b, (((0,), (0,)), ((), ())), preferred_element_type=F32)
        return 0

    lax.fori_loop(0, nz, gram_step, 0)
    for p in range(2):
        gram = gm[p]
        hi = gram.astype(BF16)
        gb[p, 0] = hi
        gb[p, 1] = (gram - hi.astype(F32)).astype(BF16)
    drain(ry, ay_recv)
    total = sb[:, y].astype(F32)
    for d in range(1, ny):
        total += ry[d - 1].astype(F32)
    tz[...] = total.astype(BF16)
    for d in far_first(nz):
        push(tz.at[lax.rem(z + d, nz)], rz.at[d - 1], 7, az_recv, peer_z(d))
    drain(rz, az_recv)
    small = tz[z].astype(F32)
    for d in range(1, nz):
        small += rz[d - 1].astype(F32)

    for i in range(4):
        drain(mo.at[i], m_sem.at[i])
    first = jnp.concatenate([mo[0], mo[2]], axis=0)
    second = jnp.concatenate([mo[1], mo[3]], axis=0)
    first_new = first_decay * first + (1.0 - first_decay) * small
    second_new = second_decay * second + (1.0 - second_decay) * small * small
    db[z, y] = (first_new / (jnp.sqrt(second_new) + 1e-08)).astype(BF16)
    for d in far_first(nz):
        push(db.at[z, y], db.at[z, y], 8, dz_recv, peer_z(d))
    mn[0], mn[1] = first_new[:8], second_new[:8]
    mn[2], mn[3] = first_new[8:], second_new[8:]
    if nz > 2:
        ring_wait(2)
        for s in (3,):
            if s <= nz // 2:
                ring_send(s)
    drain(db.at[pl.ds(0, nz - 1), y], dz_recv)
    for d in far_first(ny):
        push(db.at[:, y], db.at[:, y], 9, dy_recv, peer_y(d))
    if nz > 4:
        ring_wait(3)
        ring_send(4)
    drain(db.at[:, pl.ds(0, ny - 1)], dy_recv)

    directions = db[...].reshape(nz * ny, 16, db.shape[3]).astype(F32)
    sums = []
    for p in range(2):
        d32 = directions[:, 8 * p : 8 * p + 8].reshape(rank, -1)
        dd[p] = d32.astype(BF16)
        q = jnp.dot(gb[p, 0], dd[p], preferred_element_type=F32)
        q += jnp.dot(gb[p, 1], dd[p], preferred_element_type=F32)
        sums.append(jnp.maximum(jnp.sum(q * d32), 0.0))
    row = lax.broadcasted_iota(jnp.int32, (8, 128), 0)
    ss[me_tp] = jnp.where(row == 0, sums[0], sums[1])
    mine = ss.at[me_tp]
    for d in far_first(nx):
        for cc in (0, 1):
            push(mine, mine, 10, ss_recv, {"tp_0": lax.rem(x + d, nx), "tp_1": cc})
    push(mine, mine, 10, ss_recv, {"tp_1": 1 - c})

    def update_step(j, _):
        for p in range(2):
            up[p, j] = jnp.dot(basis(p, j), dd[p], preferred_element_type=F32)
        return 0

    lax.fori_loop(0, nz, update_step, 0)
    ring_wait(nz // 2)
    drain(ss.at[pl.ds(0, 2 * nx - 1)], ss_recv)
    squares = ss[0]
    for t in range(1, 2 * nx):
        squares += ss[t]
    factor[...] = jnp.minimum(1.0, 1.0 / jnp.sqrt(squares / entries + 1e-06))

    drain(bb.at[c, pl.ds(0, nz - 1), 0, 0], send.at[0])
    drain(bb.at[c, :, pl.ds(0, nx - 1), 0], send.at[1])
    drain(bb.at[c, :, pl.ds(0, ny - 1)], send.at[2])
    drain(wb.at[:, z, pl.ds(0, ny - 1)], send.at[3])
    drain(wb.at[:, pl.ds(0, nz - 1)], send.at[4])
    drain(bb.at[c], send.at[5])
    drain(ry, send.at[6])
    drain(rz, send.at[7])
    drain(db.at[pl.ds(0, nz - 1), 0], send.at[8])
    drain(db.at[:, pl.ds(0, ny - 1)], send.at[9])
    drain(ss.at[pl.ds(0, 2 * nx - 1)], send.at[10])


def finish_kernel(nz, ny, up, wb, wf, mn, factor, *refs):
    outs, (ob, ck, sem) = refs[:10], refs[10:]
    z, y = lax.axis_index("fs_0"), lax.axis_index("fs_1")
    rows = up.shape[2]
    factors = (factor[0, 0], factor[1, 0])

    def put(src, dst, k):
        pltpu.make_async_copy(src, dst, sem.at[k]).start()

    for i in range(4):
        put(mn.at[i], outs[4 + i], 4 + i)
    for p in range(2):
        step = factors[p] * up[p, z, pl.ds(pl.multiple_of(y * 64, 64), 64), :]
        ob[p] = wf[p] - learn_rate * step
        ob[2 + p] = step
    for i in range(4):
        put(ob.at[i], outs[i], i)

    def copy_step(j, _):
        for p in range(2):
            step = factors[p] * up[p, j]
            ck[p, j] = (wb[p, j].reshape(step.shape).astype(F32) - learn_rate * step).astype(BF16)
            put(ck.at[p, j], outs[8 + p].at[pl.ds(pl.multiple_of(j * rows, rows), rows)], 8 + p)
        return 0

    lax.fori_loop(0, nz, copy_step, 0)
    for i in range(4):
        pltpu.make_async_copy(mn.at[i], outs[4 + i], sem.at[4 + i]).wait()
        pltpu.make_async_copy(ob.at[i], outs[i], sem.at[i]).wait()
    for p in range(2):
        pltpu.make_async_copy(ck.at[p], ck.at[p], sem.at[8 + p]).wait()


def shards(nz, ny, nx, entries, *args):
    names, shapes, held = scratch(nz, ny, nx, args[0].shape[0])
    hbm, vmem = pl.BlockSpec(memory_space=pltpu.HBM), pl.BlockSpec(memory_space=pltpu.VMEM)
    kept = pl.pallas_call(
        functools.partial(update_kernel, nz, ny, nx, entries, names),
        out_shape=held,
        in_specs=[hbm] * len(args),
        out_specs=[vmem] * len(held),
        scratch_shapes=shapes,
        compiler_params=pltpu.CompilerParams(
            collective_id=0, has_side_effects=True, vmem_limit_bytes=58 * 1024 * 1024 - 448 * 1024
        ),
    )(*args)
    w, m = args[3], args[7]
    copy = jax.ShapeDtypeStruct((w.shape[0] * nz * ny, w.shape[1]), BF16)
    outs = [jax.ShapeDtypeStruct(a.shape, F32) for a in (w,) * 4 + (m,) * 4] + [copy, copy]
    return tuple(
        pl.pallas_call(
            functools.partial(finish_kernel, nz, ny),
            out_shape=outs,
            in_specs=[vmem] * len(kept),
            out_specs=[hbm] * len(outs),
            scratch_shapes=[
                pltpu.VMEM((4,) + w.shape, F32),
                pltpu.VMEM((2, nz, ny * 64, w.shape[1]), BF16),
                pltpu.SemaphoreType.DMA((10,)),
            ],
            compiler_params=pltpu.CompilerParams(vmem_limit_bytes=16 * 1024 * 1024),
        )(*kept)
    )


def build(devices, nz, ny, nx):
    torus = Mesh(devices.reshape(nz, ny, nx, 2), FS + TP)
    entries = float(nz * ny * 64 * nx * 2 * 256)
    sharded, copied = P(FS, TP), P(None, TP)
    in_specs = (P(FS, None), sharded, sharded, sharded, sharded, P(FS, None), P(FS, None)) + (sharded,) * 4
    return jax.shard_map(
        functools.partial(shards, nz, ny, nx, entries),
        mesh=torus,
        in_specs=in_specs,
        out_specs=(sharded,) * 8 + (copied,) * 2,
        check_vma=False,
    )


def solution(mesh):
    return build(mesh.devices, 8, 4, 4)
```

```python
import functools

import jax
import jax.numpy as jnp
from jax import lax
from jax.experimental import pallas as pl
from jax.experimental.pallas import tpu as pltpu
from jax.sharding import Mesh
from jax.sharding import PartitionSpec as P

FS = ("fs_0", "fs_1")
TP = ("tp_0", "tp_1")
MESH = pl.DeviceIdType.MESH
F32, BF16 = jnp.float32, jnp.bfloat16

first_decay = 0.8
second_decay = 0.95
learn_rate = 0.01


ARGS = ("x_in", "ci_in", "cg_in", "wi_in", "wg_in", "bi_in", "bg_in", "fi_in", "si_in", "fg_in", "sg_in")
HELD = ("up", "wb", "wf", "mn", "factor")
OUTS = ("ni_out", "ng_out", "ti_out", "tg_out", "fi_out", "si_out", "fg_out", "sg_out", "ki_out", "kg_out")


def scratch(nz, ny, nx, tokens):
    rank, cols, rows = nz * ny * 8, 256, ny * 64
    vmem = {
        "xb": ((nz, tokens, rows), BF16),
        "cb": ((2, tokens, cols), BF16),
        "ct": ((2, cols, tokens), BF16),
        "gg": ((nz, 2, 2, cols, rows), BF16),
        "gp": ((nz, 2, cols, rows), BF16),
        "st": ((2, cols, rank), F32),
        "bb": ((2, nz, ny, nx, 64 // nx, rank), BF16),
        "mo": ((4, 8, cols), F32),
        "sb": ((nz, ny, 16, cols), BF16),
        "ry": ((ny - 1, nz, 16, cols), BF16),
        "tz": ((nz, 16, cols), BF16),
        "rz": ((nz - 1, 16, cols), BF16),
        "db": ((nz, ny, 16, cols), BF16),
        "dd": ((2, rank, cols), BF16),
        "gm": ((rank, rank), F32),
        "gb": ((2, rank, rank), BF16),
        "pm": ((2, 8, cols), F32),
        "pn": ((2, 8, cols), F32),
        "dp": ((rank, cols), BF16),
        "ss": ((2 * nx, 8, 128), F32),
    }
    sems = {
        "x_sem": (nz,), "c_sem": (2,), "w_sem": (2,), "b_sem": None, "m_sem": (4,),
        "z_recv": (nz,), "mid_recv": (nz,), "last_recv": (nz,), "core_recv": (nz,),
        "ring_recv": (2, 2, nz // 2 + 1), "wy_recv": None, "ay_recv": None, "az_recv": None,
        "dz_recv": None, "dy_recv": None, "ss_recv": None,
        "gp_recv": (nz,), "pm_recv": None, "mn_recv": None, "dd_recv": None, "send": (15,),
    }
    held = {
        "up": ((2, nz, rows, cols), F32),
        "wb": ((2, nz, ny, 64, cols), BF16),
        "wf": ((2, 64, cols), F32),
        "mn": ((4, 8, cols), F32),
        "factor": ((2, 8, 128), F32),
    }
    names = tuple(vmem) + tuple(sems)
    dma = pltpu.SemaphoreType.DMA
    shapes = [pltpu.VMEM(*v) for v in vmem.values()] + [dma if v is None else dma(v) for v in sems.values()]
    return names, shapes, [pltpu.VMEM(*v) for v in held.values()]


def update_kernel(nz, ny, nx, entries, names, *refs):
    r = dict(zip(ARGS + HELD + names, refs))
    x_in, ci_in, cg_in, wi_in, wg_in, bi_in, bg_in, fi_in, si_in, fg_in, sg_in = (r[n] for n in ARGS)
    up, wb, wf, mn, factor = (r[n] for n in HELD)
    (
        xb, cb, ct, gg, gp, st, bb, mo, sb, ry, tz, rz, db, dd, gm, gb, pm, pn, dp, ss,
        x_sem, c_sem, w_sem, b_sem, m_sem, z_recv, mid_recv, last_recv, core_recv,
        ring_recv, wy_recv, ay_recv, az_recv, dz_recv, dy_recv, ss_recv,
        gp_recv, pm_recv, mn_recv, dd_recv, send,
    ) = (r[n] for n in names)
    slab, rows, rank = 64 // nx, ny * 64, st.shape[2]
    z, y = lax.axis_index("fs_0"), lax.axis_index("fs_1")
    x, c = lax.axis_index("tp_0"), lax.axis_index("tp_1")
    me_tp = x * 2 + c
    own_l = y * (1 - c) + x * c
    own_m = x * (1 - c) + y * c

    def far_first(n):
        return sorted(range(1, n), key=lambda d: -min(d, n - d))

    def zz_of(k):
        sign = 2 * lax.rem(k, 2) - 1 if not isinstance(k, int) else 2 * (k % 2) - 1
        return lax.rem(z + sign * ((k + 1) // 2) + nz, nz)

    def peer_z(d):
        return {"fs_0": lax.rem(z + d, nz)}

    def peer_y(d):
        return {"fs_1": lax.rem(y + d, ny)}

    def peer_mid(d):
        return {"fs_1": lax.rem(y + d * c, ny), "tp_0": lax.rem(x + d * (1 - c), nx)}

    def peer_last(d):
        return {"fs_1": lax.rem(y + d * (1 - c), ny), "tp_0": lax.rem(x + d * c, nx)}

    def push(src, dst, s, recv, device):
        pltpu.make_async_remote_copy(
            src_ref=src, dst_ref=dst, send_sem=send.at[s], recv_sem=recv,
            device_id=device, device_id_type=MESH,
        ).start()

    def drain(ref, sem):
        pltpu.make_async_copy(ref, ref, sem).wait()

    def pull(src, dst, sem):
        pltpu.make_async_copy(src, dst, sem).start()

    barrier = pltpu.get_barrier_semaphore()
    peers = [peer_z(d) for d in range(1, nz)] + [peer_y(d) for d in range(1, ny)]
    peers += [{"tp_0": lax.rem(x + d, nx), "tp_1": cc} for d in range(1, nx) for cc in (0, 1)]
    peers += [{"tp_1": 1 - c}]
    for device in peers:
        pl.semaphore_signal(barrier, inc=1, device_id=device, device_id_type=MESH)

    @pl.when(c == 0)
    def _():
        pull(bi_in.at[pl.ds(x * slab, slab)], bb.at[0, z, y, x], b_sem)

    @pl.when(c == 1)
    def _():
        pull(bg_in.at[pl.ds(x * slab, slab)], bb.at[1, z, x, y], b_sem)

    pull(wi_in, wf.at[0], w_sem.at[0])
    pull(wg_in, wf.at[1], w_sem.at[1])
    pull(ci_in, cb.at[0], c_sem.at[0])
    pull(cg_in, cb.at[1], c_sem.at[1])
    for k in range(nz):
        zz = zz_of(k)
        pull(x_in.at[:, pl.ds(pl.multiple_of(zz * rows, 128), rows)], xb.at[k], x_sem.at[k])
    for i, ref in enumerate((fi_in, si_in, fg_in, sg_in)):
        pull(ref, mo.at[i], m_sem.at[i])

    for p in range(2):
        drain(wf.at[p], w_sem.at[p])
        wb[p, z, y] = wf[p].astype(BF16)
    drain(bb.at[c, z, own_l, own_m], b_sem)
    tokens = cb.shape[1]
    chunk = min(256, tokens)
    for p in range(2):
        drain(cb.at[p], c_sem.at[p])

        def flip(i, _):
            at = pl.ds(pl.multiple_of(i * chunk, chunk), chunk)
            ct[p, :, at] = cb[p, at, :].T
            return 0

        lax.fori_loop(0, tokens // chunk, flip, 0)

    pl.semaphore_wait(barrier, len(peers))

    def mid_sends(k):
        zz = zz_of(k)
        for d in far_first(nx):
            block = bb.at[c, zz, own_l, own_m]
            push(block, block, 1, mid_recv.at[k], peer_mid(d))

    def last_sends(k):
        zz = zz_of(k)
        for d in far_first(ny):
            block = bb.at[c, zz, own_l]
            push(block, block, 2, last_recv.at[k], peer_last(d))

    def z_duty(k):
        drain(bb.at[c, zz_of(k), own_l, own_m], z_recv.at[k])
        mid_sends(k)

    def mid_duty(k):
        drain(bb.at[c, zz_of(k), own_l, pl.ds(0, nx - 1)], mid_recv.at[k])
        last_sends(k)

    partner = {"tp_1": 1 - c}
    own = bb.at[c, z, own_l, own_m]
    for k in range(nz - 1, 0, -1):
        sign, half = 2 * (k % 2) - 1, (k + 1) // 2
        at_peer = nz - 1 if k == nz - 1 else (k + 1 if k % 2 else k - 1)
        push(own, own, 0, z_recv.at[at_peer], peer_z((sign * half) % nz))
    mid_sends(0)
    for i in range(4):
        drain(mo.at[i], m_sem.at[i])
    push(mo.at[pl.ds(2 * (1 - c), 2)], pm, 12, pm_recv, partner)
    for d in far_first(ny):
        push(wb.at[:, z, y], wb.at[:, z, y], 3, wy_recv, peer_y(d))

    def grad_step(k, _):
        drain(xb.at[k], x_sem.at[k])
        for p in range(2):
            g = jnp.dot(ct[p], xb[k], preferred_element_type=F32)
            hi = g.astype(BF16)
            gg[k, p, 0] = hi
            gg[k, p, 1] = (g - hi.astype(F32)).astype(BF16)
        push(gg.at[k, 1 - c], gp.at[k], 11, gp_recv.at[k], partner)
        return 0

    def each(first, last, duty):
        def one(k, _):
            duty(k)
            return 0

        lax.fori_loop(first, last, one, 0)

    cut1, cut2 = (nz * 5) // 8, (nz * 6) // 8
    lax.fori_loop(0, cut1, grad_step, 0)
    each(1, cut1, z_duty)
    mid_duty(0)
    lax.fori_loop(cut1, cut2, grad_step, 0)
    each(cut1, nz, z_duty)
    lax.fori_loop(cut2, nz, grad_step, 0)
    each(1, nz, mid_duty)

    def ring_reach(p, way):
        return nz // 2 if p == way else nz - 1 - nz // 2

    def ring_block(p, way, s):
        return wb.at[p, lax.rem(z - s + nz if way == 0 else z + s, nz)]

    def ring_send(s):
        for p in range(2):
            for way in range(2):
                if s <= ring_reach(p, way):
                    block = ring_block(p, way, s - 1)
                    push(block, block, 4, ring_recv.at[p, way, s], peer_z(1 if way == 0 else nz - 1))

    def ring_wait(s):
        for p in range(2):
            for way in range(2):
                if s <= ring_reach(p, way):
                    drain(ring_block(p, way, s), ring_recv.at[p, way, s])

    drain(wb.at[:, z, pl.ds(0, ny - 1)], wy_recv)
    ring_send(1)

    def basis(p, j):
        if p == 0:
            return bb[0, j].reshape(rows, rank)
        b = bb[1, j]
        return jnp.concatenate([b[l, m] for m in range(ny) for l in range(nx)], axis=0)

    def own_basis(j):
        blocks = []
        for yy in range(ny):
            for xx in range(nx):
                blocks.append(bb[c, j, yy * (1 - c) + xx * c, xx * (1 - c) + yy * c])
        return jnp.concatenate(blocks, axis=0)

    st[...] = jnp.zeros_like(st)

    def small_step(k, _):
        zz = zz_of(k)
        drain(bb.at[c, zz, pl.ds(0, ny - 1)], last_recv.at[k])
        push(bb.at[c, zz], bb.at[c, zz], 5, core_recv.at[k], partner)
        drain(gp.at[k], gp_recv.at[k])
        b = own_basis(zz)
        for h, part in ((0, gg.at[k, c]), (1, gp.at[k])):
            st[h] += jnp.dot(part[0], b, preferred_element_type=F32) + jnp.dot(
                part[1], b, preferred_element_type=F32
            )
        return 0

    lax.fori_loop(0, nz, small_step, 0)

    parts = [st[p].T.reshape(rank // 8, 8, st.shape[1]) for p in range(2)]
    sb[...] = jnp.concatenate(parts, axis=1).astype(BF16).reshape(sb.shape)
    for d in far_first(ny):
        yy = lax.rem(y + d, ny)
        push(sb.at[:, yy], ry.at[d - 1], 6, ay_recv, peer_y(d))
    if nz > 2:
        ring_wait(1)
        ring_send(2)

    gm[...] = jnp.zeros_like(gm)

    def gram_step(j, _):
        b = bb[c, j].reshape(rows, rank)
        gm[...] += lax.dot_general(b, b, (((0,), (0,)), ((), ())), preferred_element_type=F32)
        return 0

    lax.fori_loop(0, nz, gram_step, 0)
    gram = gm[...]
    hi = gram.astype(BF16)
    gb[0] = hi
    gb[1] = (gram - hi.astype(F32)).astype(BF16)
    drain(ry, ay_recv)
    total = sb[:, y].astype(F32)
    for d in range(1, ny):
        total += ry[d - 1].astype(F32)
    tz[...] = total.astype(BF16)
    for d in far_first(nz):
        push(tz.at[lax.rem(z + d, nz)], rz.at[d - 1], 7, az_recv, peer_z(d))
    drain(rz, az_recv)
    small = tz[z].astype(F32)
    for d in range(1, nz):
        small += rz[d - 1].astype(F32)

    drain(pm, pm_recv)
    first = jnp.concatenate([mo[2 * c], pm[0]], axis=0)
    second = jnp.concatenate([mo[2 * c + 1], pm[1]], axis=0)
    first_new = first_decay * first + (1.0 - first_decay) * small
    second_new = second_decay * second + (1.0 - second_decay) * small * small
    db[z, y] = (first_new / (jnp.sqrt(second_new) + 1e-08)).astype(BF16)
    for d in far_first(nz):
        push(db.at[z, y], db.at[z, y], 8, dz_recv, peer_z(d))
    mn[2 * c], mn[2 * c + 1] = first_new[:8], second_new[:8]
    pn[0], pn[1] = first_new[8:], second_new[8:]
    push(pn, mn.at[pl.ds(2 * c, 2)], 13, mn_recv, partner)
    if nz > 2:
        ring_wait(2)
        for s in (3,):
            if s <= nz // 2:
                ring_send(s)
    drain(db.at[pl.ds(0, nz - 1), y], dz_recv)
    for d in far_first(ny):
        push(db.at[:, y], db.at[:, y], 9, dy_recv, peer_y(d))
    if nz > 4:
        ring_wait(3)
        ring_send(4)
    drain(db.at[:, pl.ds(0, ny - 1)], dy_recv)

    directions = db[...].reshape(nz * ny, 16, db.shape[3]).astype(F32)
    d_own, d_other = (directions[:, 8 * h : 8 * h + 8].reshape(rank, -1) for h in range(2))
    dd[c] = d_own.astype(BF16)
    dp[...] = d_other.astype(BF16)
    push(dp, dd.at[c], 14, dd_recv, partner)
    total = jnp.zeros((rank, db.shape[3]), F32)
    for d32, dh in ((d_own, dd[c]), (d_other, dp[...])):
        q = jnp.dot(gb[0], dh, preferred_element_type=F32)
        q += jnp.dot(gb[1], dh, preferred_element_type=F32)
        total += q * d32
    ss[me_tp] = jnp.full((8, 128), jnp.maximum(jnp.sum(total), 0.0), F32)
    mine = ss.at[me_tp]
    for d in far_first(nx):
        for cc in (0, 1):
            push(mine, mine, 10, ss_recv, {"tp_0": lax.rem(x + d, nx), "tp_1": cc})
    push(mine, mine, 10, ss_recv, {"tp_1": 1 - c})

    for k in range(nz):
        drain(bb.at[1 - c, zz_of(k)], core_recv.at[k])
    drain(dd.at[1 - c], dd_recv)

    def update_step(j, _):
        for p in range(2):
            up[p, j] = jnp.dot(basis(p, j), dd[p], preferred_element_type=F32)
        return 0

    lax.fori_loop(0, nz, update_step, 0)
    ring_wait(nz // 2)
    drain(ss.at[pl.ds(0, 2 * nx - 1)], ss_recv)
    for p in range(2):
        squares = ss[p]
        for t in range(1, nx):
            squares += ss[2 * t + p]
        factor[p] = jnp.minimum(1.0, 1.0 / jnp.sqrt(squares / entries + 1e-06))
    drain(mn.at[pl.ds(2 * (1 - c), 2)], mn_recv)

    drain(bb.at[c, pl.ds(0, nz - 1), 0, 0], send.at[0])
    drain(bb.at[c, :, pl.ds(0, nx - 1), 0], send.at[1])
    drain(bb.at[c, :, pl.ds(0, ny - 1)], send.at[2])
    drain(wb.at[:, z, pl.ds(0, ny - 1)], send.at[3])
    drain(wb.at[:, pl.ds(0, nz - 1)], send.at[4])
    drain(bb.at[c], send.at[5])
    drain(ry, send.at[6])
    drain(rz, send.at[7])
    drain(db.at[pl.ds(0, nz - 1), 0], send.at[8])
    drain(db.at[:, pl.ds(0, ny - 1)], send.at[9])
    drain(ss.at[pl.ds(0, 2 * nx - 1)], send.at[10])
    drain(gp, send.at[11])
    drain(pm, send.at[12])
    drain(pn, send.at[13])
    drain(dp, send.at[14])


def finish_kernel(nz, ny, up, wb, wf, mn, factor, *refs):
    outs, (ob, ck, sem) = refs[:10], refs[10:]
    z, y = lax.axis_index("fs_0"), lax.axis_index("fs_1")
    rows = up.shape[2]
    factors = (factor[0, 0, 0], factor[1, 0, 0])

    def put(src, dst, k):
        pltpu.make_async_copy(src, dst, sem.at[k]).start()

    for i in range(4):
        put(mn.at[i], outs[4 + i], 4 + i)
    for p in range(2):
        step = factors[p] * up[p, z, pl.ds(pl.multiple_of(y * 64, 64), 64), :]
        ob[p] = wf[p] - learn_rate * step
        ob[2 + p] = step
    for i in range(4):
        put(ob.at[i], outs[i], i)

    def copy_step(j, _):
        for p in range(2):
            step = factors[p] * up[p, j]
            ck[p, j] = (wb[p, j].reshape(step.shape).astype(F32) - learn_rate * step).astype(BF16)
            put(ck.at[p, j], outs[8 + p].at[pl.ds(pl.multiple_of(j * rows, rows), rows)], 8 + p)
        return 0

    lax.fori_loop(0, nz, copy_step, 0)
    for i in range(4):
        pltpu.make_async_copy(mn.at[i], outs[4 + i], sem.at[4 + i]).wait()
        pltpu.make_async_copy(ob.at[i], outs[i], sem.at[i]).wait()
    for p in range(2):
        pltpu.make_async_copy(ck.at[p], ck.at[p], sem.at[8 + p]).wait()


def shards(nz, ny, nx, entries, *args):
    names, shapes, held = scratch(nz, ny, nx, args[0].shape[0])
    hbm, vmem = pl.BlockSpec(memory_space=pltpu.HBM), pl.BlockSpec(memory_space=pltpu.VMEM)
    kept = pl.pallas_call(
        functools.partial(update_kernel, nz, ny, nx, entries, names),
        out_shape=held,
        in_specs=[hbm] * len(args),
        out_specs=[vmem] * len(held),
        scratch_shapes=shapes,
        compiler_params=pltpu.CompilerParams(
            collective_id=0, has_side_effects=True, vmem_limit_bytes=58 * 1024 * 1024 - 448 * 1024
        ),
    )(*args)
    w, m = args[3], args[7]
    copy = jax.ShapeDtypeStruct((w.shape[0] * nz * ny, w.shape[1]), BF16)
    outs = [jax.ShapeDtypeStruct(a.shape, F32) for a in (w,) * 4 + (m,) * 4] + [copy, copy]
    return tuple(
        pl.pallas_call(
            functools.partial(finish_kernel, nz, ny),
            out_shape=outs,
            in_specs=[vmem] * len(kept),
            out_specs=[hbm] * len(outs),
            scratch_shapes=[
                pltpu.VMEM((4,) + w.shape, F32),
                pltpu.VMEM((2, nz, ny * 64, w.shape[1]), BF16),
                pltpu.SemaphoreType.DMA((10,)),
            ],
            compiler_params=pltpu.CompilerParams(vmem_limit_bytes=16 * 1024 * 1024),
        )(*kept)
    )


def build(devices, nz, ny, nx):
    torus = Mesh(devices.reshape(nz, ny, nx, 2), FS + TP)
    entries = float(nz * ny * 64 * nx * 2 * 256)
    sharded, copied = P(FS, TP), P(None, TP)
    in_specs = (P(FS, None), sharded, sharded, sharded, sharded, P(FS, None), P(FS, None)) + (sharded,) * 4
    return jax.shard_map(
        functools.partial(shards, nz, ny, nx, entries),
        mesh=torus,
        in_specs=in_specs,
        out_specs=(sharded,) * 8 + (copied,) * 2,
        check_vma=False,
    )


def solution(mesh):
    return build(mesh.devices, 8, 4, 4)
```

```python
import functools

import jax
import jax.numpy as jnp
from jax import lax
from jax.experimental import pallas as pl
from jax.experimental.pallas import tpu as pltpu
from jax.sharding import Mesh
from jax.sharding import PartitionSpec as P

FS = ("fs_0", "fs_1")
TP = ("tp_0", "tp_1")
MESH = pl.DeviceIdType.MESH
F32, BF16 = jnp.float32, jnp.bfloat16

first_decay = 0.8
second_decay = 0.95
learn_rate = 0.01


ARGS = ("x_in", "ci_in", "cg_in", "wi_in", "wg_in", "bi_in", "bg_in", "fi_in", "si_in", "fg_in", "sg_in")
HELD = ("up", "wb", "wf", "mn", "factor")
OUTS = ("ni_out", "ng_out", "ti_out", "tg_out", "fi_out", "si_out", "fg_out", "sg_out", "ki_out", "kg_out")


def scratch(nz, ny, nx, tokens):
    rank, cols, rows = nz * ny * 8, 256, ny * 64
    vmem = {
        "xb": ((nz, tokens, rows), BF16),
        "cb": ((2, tokens, cols), BF16),
        "ct": ((2, cols, tokens), BF16),
        "gg": ((nz, 2, 2, cols, rows), BF16),
        "gp": ((nz, 2, cols, rows), BF16),
        "st": ((2, cols, rank), F32),
        "bb": ((2, nz, ny, nx, 64 // nx, rank), BF16),
        "mo": ((4, 8, cols), F32),
        "sb": ((nz, ny, 16, cols), BF16),
        "ry": ((ny - 1, nz, 16, cols), BF16),
        "tz": ((nz, 16, cols), BF16),
        "rz": ((nz - 1, 16, cols), BF16),
        "db": ((nz, ny, 16, cols), BF16),
        "dd": ((2, rank, cols), BF16),
        "gm": ((rank, rank), F32),
        "gb": ((2, rank, rank), BF16),
        "pm": ((2, 8, cols), F32),
        "pn": ((2, 8, cols), F32),
        "dp": ((rank, cols), BF16),
        "ss": ((2 * nx, 8, 128), F32),
    }
    sems = {
        "x_sem": (nz,), "c_sem": (2,), "w_sem": (2,), "b_sem": None, "m_sem": (4,),
        "z_recv": (nz,), "mid_recv": (nz,), "last_recv": (nz,), "core_recv": (nz,),
        "ring_recv": (2, 2, nz // 2 + 1), "wy_recv": None, "ay_recv": None, "az_recv": None,
        "dz_recv": None, "dy_recv": None, "ss_recv": None,
        "gp_recv": (nz,), "pm_recv": None, "mn_recv": None, "dd_recv": None, "send": (15,),
    }
    held = {
        "up": ((2, nz, rows, cols), F32),
        "wb": ((2, nz, ny, 64, cols), BF16),
        "wf": ((2, 64, cols), F32),
        "mn": ((4, 8, cols), F32),
        "factor": ((2, 8, 128), F32),
    }
    names = tuple(vmem) + tuple(sems)
    dma = pltpu.SemaphoreType.DMA
    shapes = [pltpu.VMEM(*v) for v in vmem.values()] + [dma if v is None else dma(v) for v in sems.values()]
    return names, shapes, [pltpu.VMEM(*v) for v in held.values()]


def update_kernel(nz, ny, nx, entries, names, *refs):
    r = dict(zip(ARGS + HELD + names, refs))
    x_in, ci_in, cg_in, wi_in, wg_in, bi_in, bg_in, fi_in, si_in, fg_in, sg_in = (r[n] for n in ARGS)
    up, wb, wf, mn, factor = (r[n] for n in HELD)
    (
        xb, cb, ct, gg, gp, st, bb, mo, sb, ry, tz, rz, db, dd, gm, gb, pm, pn, dp, ss,
        x_sem, c_sem, w_sem, b_sem, m_sem, z_recv, mid_recv, last_recv, core_recv,
        ring_recv, wy_recv, ay_recv, az_recv, dz_recv, dy_recv, ss_recv,
        gp_recv, pm_recv, mn_recv, dd_recv, send,
    ) = (r[n] for n in names)
    slab, rows, rank = 64 // nx, ny * 64, st.shape[2]
    z, y = lax.axis_index("fs_0"), lax.axis_index("fs_1")
    x, c = lax.axis_index("tp_0"), lax.axis_index("tp_1")
    me_tp = x * 2 + c
    own_l = y * (1 - c) + x * c
    own_m = x * (1 - c) + y * c

    def far_first(n):
        return sorted(range(1, n), key=lambda d: -min(d, n - d))

    def zz_of(k):
        sign = 2 * lax.rem(k, 2) - 1 if not isinstance(k, int) else 2 * (k % 2) - 1
        return lax.rem(z + sign * ((k + 1) // 2) + nz, nz)

    def peer_z(d):
        return {"fs_0": lax.rem(z + d, nz)}

    def peer_y(d):
        return {"fs_1": lax.rem(y + d, ny)}

    def peer_mid(d):
        return {"fs_1": lax.rem(y + d * c, ny), "tp_0": lax.rem(x + d * (1 - c), nx)}

    def peer_last(d):
        return {"fs_1": lax.rem(y + d * (1 - c), ny), "tp_0": lax.rem(x + d * c, nx)}

    def push(src, dst, s, recv, device):
        pltpu.make_async_remote_copy(
            src_ref=src, dst_ref=dst, send_sem=send.at[s], recv_sem=recv,
            device_id=device, device_id_type=MESH,
        ).start()

    def drain(ref, sem):
        pltpu.make_async_copy(ref, ref, sem).wait()

    def pull(src, dst, sem):
        pltpu.make_async_copy(src, dst, sem).start()

    barrier = pltpu.get_barrier_semaphore()
    peers = [peer_z(d) for d in range(1, nz)] + [peer_y(d) for d in range(1, ny)]
    peers += [{"tp_0": lax.rem(x + d, nx), "tp_1": cc} for d in range(1, nx) for cc in (0, 1)]
    peers += [{"tp_1": 1 - c}]
    for device in peers:
        pl.semaphore_signal(barrier, inc=1, device_id=device, device_id_type=MESH)

    @pl.when(c == 0)
    def _():
        pull(bi_in.at[pl.ds(x * slab, slab)], bb.at[0, z, y, x], b_sem)

    @pl.when(c == 1)
    def _():
        pull(bg_in.at[pl.ds(x * slab, slab)], bb.at[1, z, x, y], b_sem)

    pull(wi_in, wf.at[0], w_sem.at[0])
    pull(wg_in, wf.at[1], w_sem.at[1])
    pull(ci_in, cb.at[0], c_sem.at[0])
    pull(cg_in, cb.at[1], c_sem.at[1])
    for k in range(nz):
        zz = zz_of(k)
        pull(x_in.at[:, pl.ds(pl.multiple_of(zz * rows, 128), rows)], xb.at[k], x_sem.at[k])
    for i, ref in enumerate((fi_in, si_in, fg_in, sg_in)):
        pull(ref, mo.at[i], m_sem.at[i])

    for p in range(2):
        drain(wf.at[p], w_sem.at[p])
        wb[p, z, y] = wf[p].astype(BF16)
    drain(bb.at[c, z, own_l, own_m], b_sem)
    tokens = cb.shape[1]
    chunk = min(256, tokens)
    for p in range(2):
        drain(cb.at[p], c_sem.at[p])

        def flip(i, _):
            at = pl.ds(pl.multiple_of(i * chunk, chunk), chunk)
            ct[p, :, at] = cb[p, at, :].T
            return 0

        lax.fori_loop(0, tokens // chunk, flip, 0)

    pl.semaphore_wait(barrier, len(peers))

    def mid_sends(k):
        zz = zz_of(k)
        for d in far_first(nx):
            block = bb.at[c, zz, own_l, own_m]
            push(block, block, 1, mid_recv.at[k], peer_mid(d))

    def last_sends(k):
        zz = zz_of(k)
        for d in far_first(ny):
            block = bb.at[c, zz, own_l]
            push(block, block, 2, last_recv.at[k], peer_last(d))

    def z_duty(k):
        drain(bb.at[c, zz_of(k), own_l, own_m], z_recv.at[k])
        mid_sends(k)

    def mid_duty(k):
        drain(bb.at[c, zz_of(k), own_l, pl.ds(0, nx - 1)], mid_recv.at[k])
        last_sends(k)

    partner = {"tp_1": 1 - c}
    own = bb.at[c, z, own_l, own_m]
    for k in range(nz - 1, 0, -1):
        sign, half = 2 * (k % 2) - 1, (k + 1) // 2
        at_peer = nz - 1 if k == nz - 1 else (k + 1 if k % 2 else k - 1)
        push(own, own, 0, z_recv.at[at_peer], peer_z((sign * half) % nz))
    mid_sends(0)
    for i in range(4):
        drain(mo.at[i], m_sem.at[i])
    push(mo.at[pl.ds(2 * (1 - c), 2)], pm, 12, pm_recv, partner)
    for d in far_first(ny):
        push(wb.at[:, z, y], wb.at[:, z, y], 3, wy_recv, peer_y(d))

    def grad_step(k, _):
        drain(xb.at[k], x_sem.at[k])
        for p in range(2):
            g = jnp.dot(ct[p], xb[k], preferred_element_type=F32)
            hi = g.astype(BF16)
            gg[k, p, 0] = hi
            gg[k, p, 1] = (g - hi.astype(F32)).astype(BF16)
        push(gg.at[k, 1 - c], gp.at[k], 11, gp_recv.at[k], partner)
        return 0

    def each(first, last, duty):
        def one(k, _):
            duty(k)
            return 0

        lax.fori_loop(first, last, one, 0)

    cut1, cut2, cut3 = max(1, nz // 4), nz // 2, max(1, nz * 3 // 8)
    lax.fori_loop(0, cut1, grad_step, 0)
    each(1, cut1, z_duty)
    mid_duty(0)
    lax.fori_loop(cut1, cut2, grad_step, 0)
    each(cut1, nz, z_duty)
    lax.fori_loop(cut2, nz, grad_step, 0)
    each(1, cut3, mid_duty)

    def ring_reach(p, way):
        return nz // 2 if p == way else nz - 1 - nz // 2

    def ring_block(p, way, s):
        return wb.at[p, lax.rem(z - s + nz if way == 0 else z + s, nz)]

    def ring_send(s):
        for p in range(2):
            for way in range(2):
                if s <= ring_reach(p, way):
                    block = ring_block(p, way, s - 1)
                    push(block, block, 4, ring_recv.at[p, way, s], peer_z(1 if way == 0 else nz - 1))

    def ring_wait(s):
        for p in range(2):
            for way in range(2):
                if s <= ring_reach(p, way):
                    drain(ring_block(p, way, s), ring_recv.at[p, way, s])

    drain(wb.at[:, z, pl.ds(0, ny - 1)], wy_recv)
    ring_send(1)
    each(cut3, nz, mid_duty)


    def basis(p, j):
        if p == 0:
            return bb[0, j].reshape(rows, rank)
        b = bb[1, j]
        return jnp.concatenate([b[l, m] for m in range(ny) for l in range(nx)], axis=0)

    def own_basis(j):
        blocks = []
        for yy in range(ny):
            for xx in range(nx):
                blocks.append(bb[c, j, yy * (1 - c) + xx * c, xx * (1 - c) + yy * c])
        return jnp.concatenate(blocks, axis=0)

    st[...] = jnp.zeros_like(st)

    def small_step(k, _):
        zz = zz_of(k)
        drain(bb.at[c, zz, pl.ds(0, ny - 1)], last_recv.at[k])
        push(bb.at[c, zz], bb.at[c, zz], 5, core_recv.at[k], partner)
        drain(gp.at[k], gp_recv.at[k])
        b = own_basis(zz)
        for h, part in ((0, gg.at[k, c]), (1, gp.at[k])):
            st[h] += jnp.dot(part[0], b, preferred_element_type=F32) + jnp.dot(
                part[1], b, preferred_element_type=F32
            )
        return 0

    lax.fori_loop(0, nz - 1, small_step, 0)
    if nz > 2:
        ring_wait(1)
        ring_send(2)
    lax.fori_loop(nz - 1, nz, small_step, 0)

    parts = [st[p].T.reshape(rank // 8, 8, st.shape[1]) for p in range(2)]
    sb[...] = jnp.concatenate(parts, axis=1).astype(BF16).reshape(sb.shape)
    for d in far_first(ny):
        yy = lax.rem(y + d, ny)
        push(sb.at[:, yy], ry.at[d - 1], 6, ay_recv, peer_y(d))

    gm[...] = jnp.zeros_like(gm)

    def gram_step(j, _):
        b = bb[c, j].reshape(rows, rank)
        gm[...] += lax.dot_general(b, b, (((0,), (0,)), ((), ())), preferred_element_type=F32)
        return 0

    lax.fori_loop(0, nz, gram_step, 0)
    gram = gm[...]
    hi = gram.astype(BF16)
    gb[0] = hi
    gb[1] = (gram - hi.astype(F32)).astype(BF16)
    drain(ry, ay_recv)
    total = sb[:, y].astype(F32)
    for d in range(1, ny):
        total += ry[d - 1].astype(F32)
    tz[...] = total.astype(BF16)
    for d in far_first(nz):
        push(tz.at[lax.rem(z + d, nz)], rz.at[d - 1], 7, az_recv, peer_z(d))
    drain(rz, az_recv)
    small = tz[z].astype(F32)
    for d in range(1, nz):
        small += rz[d - 1].astype(F32)

    drain(pm, pm_recv)
    first = jnp.concatenate([mo[2 * c], pm[0]], axis=0)
    second = jnp.concatenate([mo[2 * c + 1], pm[1]], axis=0)
    first_new = first_decay * first + (1.0 - first_decay) * small
    second_new = second_decay * second + (1.0 - second_decay) * small * small
    db[z, y] = (first_new / (jnp.sqrt(second_new) + 1e-08)).astype(BF16)
    for d in far_first(nz):
        push(db.at[z, y], db.at[z, y], 8, dz_recv, peer_z(d))
    mn[2 * c], mn[2 * c + 1] = first_new[:8], second_new[:8]
    pn[0], pn[1] = first_new[8:], second_new[8:]
    push(pn, mn.at[pl.ds(2 * c, 2)], 13, mn_recv, partner)
    if nz > 2:
        ring_wait(2)
        for s in (3,):
            if s <= nz // 2:
                ring_send(s)
    drain(db.at[pl.ds(0, nz - 1), y], dz_recv)
    for d in far_first(ny):
        push(db.at[:, y], db.at[:, y], 9, dy_recv, peer_y(d))
    if nz > 4:
        ring_wait(3)
        ring_send(4)
    drain(db.at[:, pl.ds(0, ny - 1)], dy_recv)

    directions = db[...].reshape(nz * ny, 16, db.shape[3]).astype(F32)
    d_own, d_other = (directions[:, 8 * h : 8 * h + 8].reshape(rank, -1) for h in range(2))
    dd[c] = d_own.astype(BF16)
    dp[...] = d_other.astype(BF16)
    push(dp, dd.at[c], 14, dd_recv, partner)
    total = jnp.zeros((rank, db.shape[3]), F32)
    for d32, dh in ((d_own, dd[c]), (d_other, dp[...])):
        q = jnp.dot(gb[0], dh, preferred_element_type=F32)
        q += jnp.dot(gb[1], dh, preferred_element_type=F32)
        total += q * d32
    ss[me_tp] = jnp.full((8, 128), jnp.maximum(jnp.sum(total), 0.0), F32)
    mine = ss.at[me_tp]
    for d in far_first(nx):
        for cc in (0, 1):
            push(mine, mine, 10, ss_recv, {"tp_0": lax.rem(x + d, nx), "tp_1": cc})
    push(mine, mine, 10, ss_recv, {"tp_1": 1 - c})

    for k in range(nz):
        drain(bb.at[1 - c, zz_of(k)], core_recv.at[k])
    drain(dd.at[1 - c], dd_recv)

    def update_step(j, _):
        for p in range(2):
            up[p, j] = jnp.dot(basis(p, j), dd[p], preferred_element_type=F32)
        return 0

    lax.fori_loop(0, nz, update_step, 0)
    ring_wait(nz // 2)
    drain(ss.at[pl.ds(0, 2 * nx - 1)], ss_recv)
    for p in range(2):
        squares = ss[p]
        for t in range(1, nx):
            squares += ss[2 * t + p]
        factor[p] = jnp.minimum(1.0, 1.0 / jnp.sqrt(squares / entries + 1e-06))
    drain(mn.at[pl.ds(2 * (1 - c), 2)], mn_recv)

    drain(bb.at[c, pl.ds(0, nz - 1), 0, 0], send.at[0])
    drain(bb.at[c, :, pl.ds(0, nx - 1), 0], send.at[1])
    drain(bb.at[c, :, pl.ds(0, ny - 1)], send.at[2])
    drain(wb.at[:, z, pl.ds(0, ny - 1)], send.at[3])
    drain(wb.at[:, pl.ds(0, nz - 1)], send.at[4])
    drain(bb.at[c], send.at[5])
    drain(ry, send.at[6])
    drain(rz, send.at[7])
    drain(db.at[pl.ds(0, nz - 1), 0], send.at[8])
    drain(db.at[:, pl.ds(0, ny - 1)], send.at[9])
    drain(ss.at[pl.ds(0, 2 * nx - 1)], send.at[10])
    drain(gp, send.at[11])
    drain(pm, send.at[12])
    drain(pn, send.at[13])
    drain(dp, send.at[14])


def finish_kernel(nz, ny, up, wb, wf, mn, factor, *refs):
    outs, (ob, ck, sem) = refs[:10], refs[10:]
    z, y = lax.axis_index("fs_0"), lax.axis_index("fs_1")
    rows = up.shape[2]
    factors = (factor[0, 0, 0], factor[1, 0, 0])

    def put(src, dst, k):
        pltpu.make_async_copy(src, dst, sem.at[k]).start()

    for i in range(4):
        put(mn.at[i], outs[4 + i], 4 + i)
    for p in range(2):
        step = factors[p] * up[p, z, pl.ds(pl.multiple_of(y * 64, 64), 64), :]
        ob[p] = wf[p] - learn_rate * step
        ob[2 + p] = step
    for i in range(4):
        put(ob.at[i], outs[i], i)

    def copy_step(j, _):
        for p in range(2):
            step = factors[p] * up[p, j]
            ck[p, j] = (wb[p, j].reshape(step.shape).astype(F32) - learn_rate * step).astype(BF16)
            put(ck.at[p, j], outs[8 + p].at[pl.ds(pl.multiple_of(j * rows, rows), rows)], 8 + p)
        return 0

    lax.fori_loop(0, nz, copy_step, 0)
    for i in range(4):
        pltpu.make_async_copy(mn.at[i], outs[4 + i], sem.at[4 + i]).wait()
        pltpu.make_async_copy(ob.at[i], outs[i], sem.at[i]).wait()
    for p in range(2):
        pltpu.make_async_copy(ck.at[p], ck.at[p], sem.at[8 + p]).wait()


def shards(nz, ny, nx, entries, *args):
    names, shapes, held = scratch(nz, ny, nx, args[0].shape[0])
    hbm, vmem = pl.BlockSpec(memory_space=pltpu.HBM), pl.BlockSpec(memory_space=pltpu.VMEM)
    kept = pl.pallas_call(
        functools.partial(update_kernel, nz, ny, nx, entries, names),
        out_shape=held,
        in_specs=[hbm] * len(args),
        out_specs=[vmem] * len(held),
        scratch_shapes=shapes,
        compiler_params=pltpu.CompilerParams(
            collective_id=0, has_side_effects=True, vmem_limit_bytes=58 * 1024 * 1024 - 448 * 1024
        ),
    )(*args)
    w, m = args[3], args[7]
    copy = jax.ShapeDtypeStruct((w.shape[0] * nz * ny, w.shape[1]), BF16)
    outs = [jax.ShapeDtypeStruct(a.shape, F32) for a in (w,) * 4 + (m,) * 4] + [copy, copy]
    return tuple(
        pl.pallas_call(
            functools.partial(finish_kernel, nz, ny),
            out_shape=outs,
            in_specs=[vmem] * len(kept),
            out_specs=[hbm] * len(outs),
            scratch_shapes=[
                pltpu.VMEM((4,) + w.shape, F32),
                pltpu.VMEM((2, nz, ny * 64, w.shape[1]), BF16),
                pltpu.SemaphoreType.DMA((10,)),
            ],
            compiler_params=pltpu.CompilerParams(vmem_limit_bytes=16 * 1024 * 1024),
        )(*kept)
    )


def build(devices, nz, ny, nx):
    torus = Mesh(devices.reshape(nz, ny, nx, 2), FS + TP)
    entries = float(nz * ny * 64 * nx * 2 * 256)
    sharded, copied = P(FS, TP), P(None, TP)
    in_specs = (P(FS, None), sharded, sharded, sharded, sharded, P(FS, None), P(FS, None)) + (sharded,) * 4
    return jax.shard_map(
        functools.partial(shards, nz, ny, nx, entries),
        mesh=torus,
        in_specs=in_specs,
        out_specs=(sharded,) * 8 + (copied,) * 2,
        check_vma=False,
    )


def solution(mesh):
    return build(mesh.devices, 8, 4, 4)
```

```python
import functools

import jax
import jax.numpy as jnp
from jax import lax
from jax.experimental import pallas as pl
from jax.experimental.pallas import tpu as pltpu
from jax.sharding import Mesh
from jax.sharding import PartitionSpec as P

FS = ("fs_0", "fs_1")
TP = ("tp_0", "tp_1")
MESH = pl.DeviceIdType.MESH
F32, BF16 = jnp.float32, jnp.bfloat16

first_decay = 0.8
second_decay = 0.95
learn_rate = 0.01


ARGS = ("x_in", "ci_in", "cg_in", "wi_in", "wg_in", "bi_in", "bg_in", "fi_in", "si_in", "fg_in", "sg_in")
HELD = ("up", "wb", "wf", "mn", "factor")
OUTS = ("ni_out", "ng_out", "ti_out", "tg_out", "fi_out", "si_out", "fg_out", "sg_out", "ki_out", "kg_out")


def scratch(nz, ny, nx, tokens):
    rank, cols, rows = nz * ny * 8, 256, ny * 64
    vmem = {
        "xb": ((nz, tokens, rows), BF16),
        "cb": ((2, tokens, cols), BF16),
        "ct": ((2, cols, tokens), BF16),
        "gg": ((nz, 2, 2, cols, rows), BF16),
        "gp": ((nz, 2, cols, rows), BF16),
        "st": ((2, cols, rank), F32),
        "bb": ((2, nz, ny, nx, 64 // nx, rank), BF16),
        "mo": ((4, 8, cols), F32),
        "sb": ((nz, ny, 16, cols), BF16),
        "ry": ((ny - 1, nz, 16, cols), BF16),
        "tz": ((nz, 16, cols), BF16),
        "rz": ((nz - 1, 16, cols), BF16),
        "db": ((nz, ny, 16, cols), BF16),
        "dd": ((2, rank, cols), BF16),
        "gm": ((rank, rank), F32),
        "gb": ((2, rank, rank), BF16),
        "pm": ((2, 8, cols), F32),
        "pn": ((2, 8, cols), F32),
        "dp": ((rank, cols), BF16),
        "ss": ((2 * nx, 8, 128), F32),
    }
    sems = {
        "x_sem": (nz,), "c_sem": (2,), "w_sem": (2,), "b_sem": None, "m_sem": (4,),
        "z_recv": (nz,), "mid_recv": (nz,), "last_recv": (nz,), "core_recv": (nz,),
        "ring_recv": (2, 2, nz // 2 + 1), "wy_recv": None, "ay_recv": None, "az_recv": None,
        "dz_recv": (nz,), "dy_recv": None, "ss_recv": None,
        "gp_recv": (nz,), "pm_recv": None, "mn_recv": None, "dd_recv": None, "send": (15,),
    }
    held = {
        "up": ((2, nz, rows, cols), F32),
        "wb": ((2, nz, ny, 64, cols), BF16),
        "wf": ((2, 64, cols), F32),
        "mn": ((4, 8, cols), F32),
        "factor": ((2, 8, 128), F32),
    }
    names = tuple(vmem) + tuple(sems)
    dma = pltpu.SemaphoreType.DMA
    shapes = [pltpu.VMEM(*v) for v in vmem.values()] + [dma if v is None else dma(v) for v in sems.values()]
    return names, shapes, [pltpu.VMEM(*v) for v in held.values()]


def update_kernel(nz, ny, nx, entries, names, *refs):
    r = dict(zip(ARGS + HELD + names, refs))
    x_in, ci_in, cg_in, wi_in, wg_in, bi_in, bg_in, fi_in, si_in, fg_in, sg_in = (r[n] for n in ARGS)
    up, wb, wf, mn, factor = (r[n] for n in HELD)
    (
        xb, cb, ct, gg, gp, st, bb, mo, sb, ry, tz, rz, db, dd, gm, gb, pm, pn, dp, ss,
        x_sem, c_sem, w_sem, b_sem, m_sem, z_recv, mid_recv, last_recv, core_recv,
        ring_recv, wy_recv, ay_recv, az_recv, dz_recv, dy_recv, ss_recv,
        gp_recv, pm_recv, mn_recv, dd_recv, send,
    ) = (r[n] for n in names)
    slab, rows, rank = 64 // nx, ny * 64, st.shape[2]
    z, y = lax.axis_index("fs_0"), lax.axis_index("fs_1")
    x, c = lax.axis_index("tp_0"), lax.axis_index("tp_1")
    me_tp = x * 2 + c
    own_l = y * (1 - c) + x * c
    own_m = x * (1 - c) + y * c

    def far_first(n):
        return sorted(range(1, n), key=lambda d: -min(d, n - d))

    def far_offset(k):
        return ((2 * (k % 2) - 1) * ((k + 1) // 2)) % nz

    def far_index(k):
        return nz - 1 if k == nz - 1 else (k + 1 if k % 2 else k - 1)

    def zz_of(k):
        sign = 2 * lax.rem(k, 2) - 1 if not isinstance(k, int) else 2 * (k % 2) - 1
        return lax.rem(z + sign * ((k + 1) // 2) + nz, nz)

    def peer_z(d):
        return {"fs_0": lax.rem(z + d, nz)}

    def peer_y(d):
        return {"fs_1": lax.rem(y + d, ny)}

    def peer_mid(d):
        return {"fs_1": lax.rem(y + d * c, ny), "tp_0": lax.rem(x + d * (1 - c), nx)}

    def peer_last(d):
        return {"fs_1": lax.rem(y + d * (1 - c), ny), "tp_0": lax.rem(x + d * c, nx)}

    def push(src, dst, s, recv, device):
        pltpu.make_async_remote_copy(
            src_ref=src, dst_ref=dst, send_sem=send.at[s], recv_sem=recv,
            device_id=device, device_id_type=MESH,
        ).start()

    def drain(ref, sem):
        pltpu.make_async_copy(ref, ref, sem).wait()

    def pull(src, dst, sem):
        pltpu.make_async_copy(src, dst, sem).start()

    barrier = pltpu.get_barrier_semaphore()
    peers = [peer_z(d) for d in range(1, nz)] + [peer_y(d) for d in range(1, ny)]
    peers += [{"tp_0": lax.rem(x + d, nx), "tp_1": cc} for d in range(1, nx) for cc in (0, 1)]
    peers += [{"tp_1": 1 - c}]
    for device in peers:
        pl.semaphore_signal(barrier, inc=1, device_id=device, device_id_type=MESH)

    @pl.when(c == 0)
    def _():
        pull(bi_in.at[pl.ds(x * slab, slab)], bb.at[0, z, y, x], b_sem)

    @pl.when(c == 1)
    def _():
        pull(bg_in.at[pl.ds(x * slab, slab)], bb.at[1, z, x, y], b_sem)

    pull(wi_in, wf.at[0], w_sem.at[0])
    pull(wg_in, wf.at[1], w_sem.at[1])
    pull(ci_in, cb.at[0], c_sem.at[0])
    pull(cg_in, cb.at[1], c_sem.at[1])
    for k in range(nz):
        zz = zz_of(k)
        pull(x_in.at[:, pl.ds(pl.multiple_of(zz * rows, 128), rows)], xb.at[k], x_sem.at[k])
    for i, ref in enumerate((fi_in, si_in, fg_in, sg_in)):
        pull(ref, mo.at[i], m_sem.at[i])

    for p in range(2):
        drain(wf.at[p], w_sem.at[p])
        wb[p, z, y] = wf[p].astype(BF16)
    drain(bb.at[c, z, own_l, own_m], b_sem)
    tokens = cb.shape[1]
    chunk = min(256, tokens)
    for p in range(2):
        drain(cb.at[p], c_sem.at[p])

        def flip(i, _):
            at = pl.ds(pl.multiple_of(i * chunk, chunk), chunk)
            ct[p, :, at] = cb[p, at, :].T
            return 0

        lax.fori_loop(0, tokens // chunk, flip, 0)

    pl.semaphore_wait(barrier, len(peers))

    def mid_sends(k):
        zz = zz_of(k)
        for d in far_first(nx):
            block = bb.at[c, zz, own_l, own_m]
            push(block, block, 1, mid_recv.at[k], peer_mid(d))

    def last_sends(k):
        zz = zz_of(k)
        for d in far_first(ny):
            block = bb.at[c, zz, own_l]
            push(block, block, 2, last_recv.at[k], peer_last(d))

    def z_duty(k):
        drain(bb.at[c, zz_of(k), own_l, own_m], z_recv.at[k])
        mid_sends(k)

    def mid_duty(k):
        drain(bb.at[c, zz_of(k), own_l, pl.ds(0, nx - 1)], mid_recv.at[k])
        last_sends(k)

    partner = {"tp_1": 1 - c}
    own = bb.at[c, z, own_l, own_m]
    for k in range(nz - 1, 0, -1):
        push(own, own, 0, z_recv.at[far_index(k)], peer_z(far_offset(k)))
    mid_sends(0)
    for i in range(4):
        drain(mo.at[i], m_sem.at[i])
    push(mo.at[pl.ds(2 * (1 - c), 2)], pm, 12, pm_recv, partner)
    for d in far_first(ny):
        push(wb.at[:, z, y], wb.at[:, z, y], 3, wy_recv, peer_y(d))

    def grad_step(k, _):
        drain(xb.at[k], x_sem.at[k])
        for p in range(2):
            g = jnp.dot(ct[p], xb[k], preferred_element_type=F32)
            hi = g.astype(BF16)
            gg[k, p, 0] = hi
            gg[k, p, 1] = (g - hi.astype(F32)).astype(BF16)
        push(gg.at[k, 1 - c], gp.at[k], 11, gp_recv.at[k], partner)
        return 0

    def each(first, last, duty):
        def one(k, _):
            duty(k)
            return 0

        lax.fori_loop(first, last, one, 0)

    cut1, cut2, cut3 = max(1, nz // 4), nz // 2, max(1, nz * 3 // 8)
    lax.fori_loop(0, cut1, grad_step, 0)
    each(1, cut1, z_duty)
    mid_duty(0)
    lax.fori_loop(cut1, cut2, grad_step, 0)
    each(cut1, nz, z_duty)
    lax.fori_loop(cut2, nz, grad_step, 0)
    each(1, cut3, mid_duty)

    def ring_reach(p, way):
        return nz // 2 if p == way else nz - 1 - nz // 2

    def ring_block(p, way, s):
        return wb.at[p, lax.rem(z - s + nz if way == 0 else z + s, nz)]

    def ring_send(s):
        for p in range(2):
            for way in range(2):
                if s <= ring_reach(p, way):
                    block = ring_block(p, way, s - 1)
                    push(block, block, 4, ring_recv.at[p, way, s], peer_z(1 if way == 0 else nz - 1))

    def ring_wait(s):
        for p in range(2):
            for way in range(2):
                if s <= ring_reach(p, way):
                    drain(ring_block(p, way, s), ring_recv.at[p, way, s])

    drain(wb.at[:, z, pl.ds(0, ny - 1)], wy_recv)
    ring_send(1)
    each(cut3, nz, mid_duty)


    def basis(p, j):
        if p == 0:
            return bb[0, j].reshape(rows, rank)
        b = bb[1, j]
        return jnp.concatenate([b[l, m] for m in range(ny) for l in range(nx)], axis=0)

    def own_basis(j):
        blocks = []
        for yy in range(ny):
            for xx in range(nx):
                blocks.append(bb[c, j, yy * (1 - c) + xx * c, xx * (1 - c) + yy * c])
        return jnp.concatenate(blocks, axis=0)

    st[...] = jnp.zeros_like(st)

    def small_step(k, _):
        zz = zz_of(k)
        drain(bb.at[c, zz, pl.ds(0, ny - 1)], last_recv.at[k])
        push(bb.at[c, zz], bb.at[c, zz], 5, core_recv.at[k], partner)
        drain(gp.at[k], gp_recv.at[k])
        b = own_basis(zz)
        for h, part in ((0, gg.at[k, c]), (1, gp.at[k])):
            st[h] += jnp.dot(part[0], b, preferred_element_type=F32) + jnp.dot(
                part[1], b, preferred_element_type=F32
            )
        return 0

    lax.fori_loop(0, nz - 1, small_step, 0)
    if nz > 2:
        ring_wait(1)
        ring_send(2)
    lax.fori_loop(nz - 1, nz, small_step, 0)

    parts = [st[p].T.reshape(rank // 8, 8, st.shape[1]) for p in range(2)]
    sb[...] = jnp.concatenate(parts, axis=1).astype(BF16).reshape(sb.shape)
    for d in far_first(ny):
        yy = lax.rem(y + d, ny)
        push(sb.at[:, yy], ry.at[d - 1], 6, ay_recv, peer_y(d))

    gm[...] = jnp.zeros_like(gm)

    def gram_step(j, _):
        b = bb[c, j].reshape(rows, rank)
        gm[...] += lax.dot_general(b, b, (((0,), (0,)), ((), ())), preferred_element_type=F32)
        return 0

    lax.fori_loop(0, nz, gram_step, 0)
    gram = gm[...]
    hi = gram.astype(BF16)
    gb[0] = hi
    gb[1] = (gram - hi.astype(F32)).astype(BF16)
    drain(ry, ay_recv)
    for d in far_first(nz) + [0]:
        zz = lax.rem(z + d, nz)
        total = sb[zz, y].astype(F32)
        for e in range(1, ny):
            total += ry[e - 1, zz].astype(F32)
        tz[zz] = total.astype(BF16)
        if d:
            push(tz.at[zz], rz.at[d - 1], 7, az_recv, peer_z(d))
    drain(rz, az_recv)
    small = tz[z].astype(F32)
    for d in range(1, nz):
        small += rz[d - 1].astype(F32)

    drain(pm, pm_recv)
    first = jnp.concatenate([mo[2 * c], pm[0]], axis=0)
    second = jnp.concatenate([mo[2 * c + 1], pm[1]], axis=0)
    first_new = first_decay * first + (1.0 - first_decay) * small
    second_new = second_decay * second + (1.0 - second_decay) * small * small
    db[z, y] = (first_new / (jnp.sqrt(second_new) + 1e-08)).astype(BF16)
    for k in range(nz - 1, 0, -1):
        push(db.at[z, y], db.at[z, y], 8, dz_recv.at[far_index(k)], peer_z(far_offset(k)))

    def direction_sends(k):
        block = db.at[zz_of(k), y]
        for d in far_first(ny):
            push(block, block, 9, dy_recv, peer_y(d))

    def direction_duty(k):
        drain(db.at[zz_of(k), y], dz_recv.at[k])
        direction_sends(k)

    direction_sends(0)
    mn[2 * c], mn[2 * c + 1] = first_new[:8], second_new[:8]
    pn[0], pn[1] = first_new[8:], second_new[8:]
    push(pn, mn.at[pl.ds(2 * c, 2)], 13, mn_recv, partner)
    if nz > 2:
        ring_wait(2)
        for s in (3,):
            if s <= nz // 2:
                ring_send(s)
    each(1, nz, direction_duty)
    if nz > 4:
        ring_wait(3)
        ring_send(4)
    drain(db.at[:, pl.ds(0, ny - 1)], dy_recv)

    directions = db[...].reshape(nz * ny, 16, db.shape[3]).astype(F32)
    d_own, d_other = (directions[:, 8 * h : 8 * h + 8].reshape(rank, -1) for h in range(2))
    dd[c] = d_own.astype(BF16)
    dp[...] = d_other.astype(BF16)
    push(dp, dd.at[c], 14, dd_recv, partner)
    total = jnp.zeros((rank, db.shape[3]), F32)
    for d32, dh in ((d_own, dd[c]), (d_other, dp[...])):
        q = jnp.dot(gb[0], dh, preferred_element_type=F32)
        q += jnp.dot(gb[1], dh, preferred_element_type=F32)
        total += q * d32
    ss[me_tp] = jnp.full((8, 128), jnp.maximum(jnp.sum(total), 0.0), F32)
    mine = ss.at[me_tp]
    for d in far_first(nx):
        for cc in (0, 1):
            push(mine, mine, 10, ss_recv, {"tp_0": lax.rem(x + d, nx), "tp_1": cc})
    push(mine, mine, 10, ss_recv, {"tp_1": 1 - c})

    for k in range(nz):
        drain(bb.at[1 - c, zz_of(k)], core_recv.at[k])
    drain(dd.at[1 - c], dd_recv)

    def update_step(j, _):
        for p in range(2):
            up[p, j] = jnp.dot(basis(p, j), dd[p], preferred_element_type=F32)
        return 0

    lax.fori_loop(0, nz, update_step, 0)
    ring_wait(nz // 2)
    drain(ss.at[pl.ds(0, 2 * nx - 1)], ss_recv)
    for p in range(2):
        squares = ss[p]
        for t in range(1, nx):
            squares += ss[2 * t + p]
        factor[p] = jnp.minimum(1.0, 1.0 / jnp.sqrt(squares / entries + 1e-06))
    drain(mn.at[pl.ds(2 * (1 - c), 2)], mn_recv)

    drain(bb.at[c, pl.ds(0, nz - 1), 0, 0], send.at[0])
    drain(bb.at[c, :, pl.ds(0, nx - 1), 0], send.at[1])
    drain(bb.at[c, :, pl.ds(0, ny - 1)], send.at[2])
    drain(wb.at[:, z, pl.ds(0, ny - 1)], send.at[3])
    drain(wb.at[:, pl.ds(0, nz - 1)], send.at[4])
    drain(bb.at[c], send.at[5])
    drain(ry, send.at[6])
    drain(rz, send.at[7])
    drain(db.at[pl.ds(0, nz - 1), 0], send.at[8])
    drain(db.at[:, pl.ds(0, ny - 1)], send.at[9])
    drain(ss.at[pl.ds(0, 2 * nx - 1)], send.at[10])
    drain(gp, send.at[11])
    drain(pm, send.at[12])
    drain(pn, send.at[13])
    drain(dp, send.at[14])


def finish_kernel(nz, ny, up, wb, wf, mn, factor, *refs):
    outs, (ob, ck, sem) = refs[:10], refs[10:]
    z, y = lax.axis_index("fs_0"), lax.axis_index("fs_1")
    rows = up.shape[2]
    factors = (factor[0, 0, 0], factor[1, 0, 0])

    def put(src, dst, k):
        pltpu.make_async_copy(src, dst, sem.at[k]).start()

    for i in range(4):
        put(mn.at[i], outs[4 + i], 4 + i)
    for p in range(2):
        step = factors[p] * up[p, z, pl.ds(pl.multiple_of(y * 64, 64), 64), :]
        ob[p] = wf[p] - learn_rate * step
        ob[2 + p] = step
    for i in range(4):
        put(ob.at[i], outs[i], i)

    def copy_step(j, _):
        for p in range(2):
            step = factors[p] * up[p, j]
            ck[p, j] = (wb[p, j].reshape(step.shape).astype(F32) - learn_rate * step).astype(BF16)
            put(ck.at[p, j], outs[8 + p].at[pl.ds(pl.multiple_of(j * rows, rows), rows)], 8 + p)
        return 0

    lax.fori_loop(0, nz, copy_step, 0)
    for i in range(4):
        pltpu.make_async_copy(mn.at[i], outs[4 + i], sem.at[4 + i]).wait()
        pltpu.make_async_copy(ob.at[i], outs[i], sem.at[i]).wait()
    for p in range(2):
        pltpu.make_async_copy(ck.at[p], ck.at[p], sem.at[8 + p]).wait()


def shards(nz, ny, nx, entries, *args):
    names, shapes, held = scratch(nz, ny, nx, args[0].shape[0])
    hbm, vmem = pl.BlockSpec(memory_space=pltpu.HBM), pl.BlockSpec(memory_space=pltpu.VMEM)
    kept = pl.pallas_call(
        functools.partial(update_kernel, nz, ny, nx, entries, names),
        out_shape=held,
        in_specs=[hbm] * len(args),
        out_specs=[vmem] * len(held),
        scratch_shapes=shapes,
        compiler_params=pltpu.CompilerParams(
            collective_id=0, has_side_effects=True, vmem_limit_bytes=58 * 1024 * 1024 - 448 * 1024
        ),
    )(*args)
    w, m = args[3], args[7]
    copy = jax.ShapeDtypeStruct((w.shape[0] * nz * ny, w.shape[1]), BF16)
    outs = [jax.ShapeDtypeStruct(a.shape, F32) for a in (w,) * 4 + (m,) * 4] + [copy, copy]
    return tuple(
        pl.pallas_call(
            functools.partial(finish_kernel, nz, ny),
            out_shape=outs,
            in_specs=[vmem] * len(kept),
            out_specs=[hbm] * len(outs),
            scratch_shapes=[
                pltpu.VMEM((4,) + w.shape, F32),
                pltpu.VMEM((2, nz, ny * 64, w.shape[1]), BF16),
                pltpu.SemaphoreType.DMA((10,)),
            ],
            compiler_params=pltpu.CompilerParams(vmem_limit_bytes=16 * 1024 * 1024),
        )(*kept)
    )


def build(devices, nz, ny, nx):
    torus = Mesh(devices.reshape(nz, ny, nx, 2), FS + TP)
    entries = float(nz * ny * 64 * nx * 2 * 256)
    sharded, copied = P(FS, TP), P(None, TP)
    in_specs = (P(FS, None), sharded, sharded, sharded, sharded, P(FS, None), P(FS, None)) + (sharded,) * 4
    return jax.shard_map(
        functools.partial(shards, nz, ny, nx, entries),
        mesh=torus,
        in_specs=in_specs,
        out_specs=(sharded,) * 8 + (copied,) * 2,
        check_vma=False,
    )


def solution(mesh):
    return build(mesh.devices, 8, 4, 4)
```
